512 devices in a mesh: kv: 64 (over z, y), tp: 8 (over x, core).
Axes of the slice: x: 4, y: 4, z: 16, core: 2. Of those that a mesh axis runs over, the one named last changes fastest.
Arguments:
- tokens: bfloat16 [24576, 2048], P('kv', 'tp'), may hold values from -12 to 12
- query_weight: bfloat16 [2048, 2048], P(None, 'tp'), may hold values from -0.5 to 0.5
- key_weight: bfloat16 [2048, 1024], P(None, 'tp'), may hold values from -0.5 to 0.5
- value_weight: bfloat16 [2048, 1024], P(None, 'tp'), may hold values from -0.125 to 0.125
- out_weight: bfloat16 [2048, 2048], P(None, 'tp'), may hold values from -0.125 to 0.125
- chosen: int32 [384, 16], P('kv'), may hold values from 0 to 383, as said below
Outputs:
- mixed: bfloat16 [24576, 2048], P('kv', 'tp')
The draws below stay inside these ranges and needn't reach their ends.
Inputs may be any that keep to these rules, and one draw needn't show every extreme that they name: `chosen`: row b names no block after b; its first entry is b and its next 3 entries are blocks of the same device as block b; entries may repeat. Over the rows of one device, the entries after the first 4 name at most 2 blocks, counting repeats, of any one other device, and some device names exactly 2 of another.
All inputs are finite; a program needn't handle non-finite values.
Results may differ from the reference program's by a relative error of at most 0.0072.
Values may be sent and summed in bfloat16 or wider, within the bound.
A program may use at most 128 MiB of HBM per device.

```python
import jax
import jax.numpy as jnp
from jax import lax

D = 2048
H = 16
KVH = 8
HD = 128
BLK = 64
TOPB = 16
LOCAL = 3
CAP = 2
TOK_DEV = 384
TOKENS = 24576
NQB = 384
N_KV = 64


def draw_tokens(key, part):
    plain = jnp.clip(jax.random.normal(key, (TOKENS, D), jnp.float32), -6.0, 6.0)
    return plain.astype(jnp.bfloat16)


def draw_query_weight(key, part):
    fresh = jax.random.normal(jax.random.fold_in(key, 11), (D, H * HD), jnp.float32)
    return jnp.clip(fresh * D ** (-0.5), -0.5, 0.5).astype(jnp.bfloat16)


def draw_key_weight(key, part):
    fresh = jax.random.normal(jax.random.fold_in(key, 12), (D, KVH * HD), jnp.float32)
    return jnp.clip(fresh * D ** (-0.5), -0.5, 0.5).astype(jnp.bfloat16)


def draw_chosen(key, part):
    blocks = TOK_DEV // BLK
    far_count = TOPB - 1 - LOCAL
    ask_count = blocks * far_count
    picked = min(ask_count // CAP, N_KV)
    streams = jax.random.split(jax.random.fold_in(key, 21), 6)
    devices = jnp.arange(N_KV, dtype=jnp.int32)
    asking = devices[:, None]
    target = devices[None, :]
    raw_score = jax.random.randint(streams[0], (N_KV, N_KV), 0, 1 << 14)
    popular = jax.random.randint(streams[1], (1, N_KV), 0, 4) == 0
    forced = (target == asking - 1) | (target == asking - N_KV // 2)
    scores = raw_score * 1024 + target
    scores = scores + jnp.where(popular, 1 << 25, 0) + jnp.where(forced, 1 << 26, 0)
    scores = jnp.where(target < asking, scores, -1 - target)
    ranked = lax.top_k(scores, picked)[1].astype(jnp.int32)
    usable = jnp.minimum(devices, picked)
    request = jnp.arange(ask_count, dtype=jnp.int32)
    owner_slot = request // CAP
    holder = jnp.take_along_axis(ranked, jnp.broadcast_to(jnp.minimum(owner_slot, picked - 1)[None, :], (N_KV, ask_count)), axis=1)
    usable_slot = owner_slot[None, :] < usable[:, None]
    hot_block = jax.random.randint(streams[2], (N_KV,), 0, blocks)
    coin_flip = jax.random.randint(streams[3], (N_KV, ask_count), 0, 2)
    any_block = jax.random.randint(streams[4], (N_KV, ask_count), 0, blocks)
    inside = jnp.where(coin_flip == 0, hot_block[holder], any_block)
    query_block = devices[:, None] * blocks + request[None, :] // far_count
    far_ids = jnp.where(usable_slot, holder * blocks + inside, query_block).reshape(N_KV, blocks, far_count)
    own_ids = devices[:, None] * blocks + jnp.arange(blocks, dtype=jnp.int32)[None, :]
    near_raw = jax.random.randint(streams[5], (N_KV, blocks, LOCAL), 0, 1 << 16)
    near_ids = devices[:, None, None] * blocks + near_raw % (jnp.arange(blocks, dtype=jnp.int32)[None, :, None] + 1)
    table_rows = jnp.concatenate([own_ids[:, :, None], near_ids, far_ids], axis=2)
    return table_rows.reshape(N_KV * blocks, TOPB).astype(jnp.int32)


def steps_of(rng, extent, cuts, low, largest):
    loudness = 1.0
    for axis_at, blocks in cuts:
        steps = jax.random.uniform(jax.random.fold_in(jax.random.fold_in(rng, 6), axis_at), (blocks,), jnp.float32, low / len(cuts), largest / len(cuts))
        loudness = loudness * jnp.repeat(jnp.exp(steps), extent[axis_at] // blocks).reshape((-1,) + (1,) * (len(extent) - 1 - axis_at))
    return loudness


def centred(rng, dims, width, limit, cuts=(), kind=jnp.bfloat16):
    values = jax.random.normal(rng, dims, jnp.float32) * width
    if len(cuts) > 0:
        values = steps_of(rng, dims, cuts, -0.22, 0.18) * values
    return jnp.clip(values, min=-limit, max=limit).astype(kind)


def setup_inputs(seed: int = 0) -> dict:
    keys = jax.random.split(jax.random.key(seed), 7)
    return {
        "tokens": draw_tokens(jax.random.fold_in(keys[6], 71), 0),
        "query_weight": draw_query_weight(jax.random.fold_in(keys[6], 71), 0),
        "key_weight": draw_key_weight(jax.random.fold_in(keys[6], 71), 0),
        "value_weight": centred(keys[3], (D, KVH * HD), D ** -0.5, 0.125, ((1, 8),)),
        "out_weight": centred(keys[4], (H * HD, D), (H * HD) ** -0.5, 0.125, ((1, 8),)),
        "chosen": draw_chosen(jax.random.fold_in(keys[6], 71), 0),
    }


def reference(tokens, query_weight, key_weight, value_weight, out_weight, chosen):
    queries = jnp.dot(tokens, query_weight, preferred_element_type=jnp.float32).astype(jnp.bfloat16)
    key_rows = jnp.dot(tokens, key_weight, preferred_element_type=jnp.float32).astype(jnp.bfloat16)
    value_rows = jnp.dot(tokens, value_weight, preferred_element_type=jnp.float32).astype(jnp.bfloat16)
    group_size = H // KVH
    grouped = queries.reshape(NQB, BLK, KVH, group_size, HD)
    key_blocks = key_rows.reshape(NQB, BLK, KVH, HD)
    value_blocks = value_rows.reshape(NQB, BLK, KVH, HD)

    def attend(inputs):
        block_queries, chosen_row, block_number = inputs
        slot_order = jnp.arange(TOPB)
        repeats = jnp.any((chosen_row[:, None] == chosen_row[None, :]) & (slot_order[None, :] < slot_order[:, None]), axis=1)
        got_keys = jnp.take(key_blocks, chosen_row, axis=0).reshape(TOPB * BLK, KVH, HD)
        got_values = jnp.take(value_blocks, chosen_row, axis=0).reshape(TOPB * BLK, KVH, HD)
        scores = jnp.einsum("qkgd,skd->kgqs", block_queries.astype(jnp.float32), got_keys.astype(jnp.float32),
                            precision=lax.Precision.HIGHEST) * (HD ** -0.5)
        query_pos = block_number * BLK + jnp.arange(BLK, dtype=jnp.int32)
        key_pos = (chosen_row[:, None] * BLK + jnp.arange(BLK, dtype=jnp.int32)[None, :]).reshape(-1)
        fresh_slot = jnp.broadcast_to((~repeats)[:, None], (TOPB, BLK)).reshape(-1)
        visible = fresh_slot[None, :] & (key_pos[None, :] <= query_pos[:, None])
        scores = jnp.where(visible[None, None], scores, -jnp.inf)
        row_peak = jnp.max(scores, axis=-1, keepdims=True)
        weights = jnp.exp(scores - row_peak)
        row_total = jnp.sum(weights, axis=-1)
        rounded = lax.optimization_barrier(weights.astype(jnp.bfloat16)).astype(jnp.float32)
        mixed_heads = jnp.einsum("kgqs,skd->qkgd", rounded, got_values.astype(jnp.float32),
                                 precision=lax.Precision.HIGHEST)
        mixed_heads = mixed_heads / jnp.transpose(row_total, (2, 0, 1))[..., None]
        return mixed_heads.astype(jnp.bfloat16).reshape(BLK, H * HD)

    heads_out = lax.map(attend, (grouped, chosen, jnp.arange(NQB, dtype=jnp.int32)))
    return jnp.dot(heads_out.reshape(TOKENS, H * HD), out_weight, preferred_element_type=jnp.float32).astype(jnp.bfloat16)
```

```python
import math

import jax
import jax.numpy as jnp
from jax import lax
from jax.experimental import pallas as pl
from jax.experimental.pallas import tpu as pltpu
from jax.sharding import PartitionSpec as P

HD = 128
BLK = 64
TOPB = 16
NB = 6
NX, NY, NZ = 4, 4, 16
ROWS = NB * BLK
COLS = 256
PER = 10
OWN = NZ * PER
MESH = pl.DeviceIdType.MESH
BF = jnp.bfloat16
F32 = jnp.float32
EXP_SCALE = HD ** (-0.5) * math.log2(math.e)


class Exchange:
    def __init__(self, buf, rows, x, c, kv, ssem, rsem):
        self.buf, self.rows, self.x, self.c, self.kv = buf, rows, x, c, kv
        self.ssem, self.rsem = ssem, rsem
        self.xp, self.xm, self.xo = (x + 1) % NX, (x + NX - 1) % NX, (x + 2) % NX
        self.pc = 1 - c
        self.sent = []

    def part(self, x, c, chunk, half=None):
        rows = self.rows if half is None else self.rows // 2
        start = chunk * self.rows + (0 if half is None else half * rows)
        return self.buf.at[x * 2 + c, pl.ds(start, rows), :]

    def copy(self, ref, chunk, kind, x, c):
        return pltpu.make_async_remote_copy(
            src_ref=ref, dst_ref=ref, send_sem=self.ssem.at[chunk, kind], recv_sem=self.rsem.at[chunk, kind],
            device_id={"kv": self.kv, "tp": x * 2 + c}, device_id_type=MESH,
        )

    def send(self, ref, chunk, kind, x, c):
        copy = self.copy(ref, chunk, kind, x, c)
        copy.start()
        self.sent.append(copy)

    def got(self, ref, chunk, kind):
        self.copy(ref, chunk, kind, self.x, self.pc).wait_recv()

    def own(self, k):
        ref = self.part(self.x, self.c, k)
        self.send(ref, k, 0, self.xp, self.c)
        self.send(ref, k, 1, self.xm, self.c)
        self.send(ref, k, 2, self.x, self.pc)

    def direct(self, k):
        self.got(self.part(self.xm, self.c, k), k, 0)
        self.send(self.part(self.xm, self.c, k, 0), k, 3, self.xp, self.c)
        self.send(self.part(self.xm, self.c, k), k, 5, self.x, self.pc)
        self.got(self.part(self.xp, self.c, k), k, 1)
        self.send(self.part(self.xp, self.c, k, 1), k, 4, self.xm, self.c)
        self.send(self.part(self.xp, self.c, k), k, 6, self.x, self.pc)

    def relayed(self, k):
        for half in (0, 1):
            ref = self.part(self.xo, self.c, k, half)
            self.got(ref, k, 3 + half)
            self.send(ref, k, 7 + half, self.x, self.pc)

    def finish(self, k):
        self.got(self.part(self.x, self.pc, k), k, 2)
        self.got(self.part(self.xm, self.pc, k), k, 5)
        self.got(self.part(self.xp, self.pc, k), k, 6)
        self.got(self.part(self.xo, self.pc, k, 0), k, 7)
        self.got(self.part(self.xo, self.pc, k, 1), k, 8)

    def drain(self):
        for copy in self.sent:
            copy.wait_send()


def kernel(tok, wq, wk, wv, wo, req_in, idx_ref, bias_ref, out_ref, *scratch):
    (xbuf, hbuf, wqkv, wos, qs, own, mid, pool, stage, kvs, rbuf, req_sm) = scratch[:12]
    units_f, units_b = scratch[12:19], scratch[19:26]
    (lsem, a_s, a_r, e_s, e_r, zs, zr, ms, mr, ys, yr, os_, or_, rs, rr, smem_sem) = scratch[26:]

    kv = lax.axis_index("kv")
    tp = lax.axis_index("tp")
    z, y = kv // NY, kv % NY
    x, c = tp // 2, tp % 2
    yp, ym, yo = (y + 1) % NY, (y + NY - 1) % NY, (y + 2) % NY
    zp, zm = (z + 1) % NZ, (z + NZ - 1) % NZ

    loads = [
        pltpu.make_async_copy(tok, xbuf.at[tp], lsem.at[0]),
        pltpu.make_async_copy(wq, wqkv.at[:, 0:256], lsem.at[1]),
        pltpu.make_async_copy(wk, wqkv.at[:, 256:384], lsem.at[2]),
        pltpu.make_async_copy(wv, wqkv.at[:, 384:512], lsem.at[3]),
        pltpu.make_async_copy(wo, wos, lsem.at[4]),
    ]
    for load in loads:
        load.start()

    def dev(zz, yy, tt):
        return {"kv": zz * NY + yy, "tp": tt}

    near = [
        dev(z, y, x * 2 + 1 - c), dev(z, y, ((x + 1) % NX) * 2 + c), dev(z, y, ((x + 3) % NX) * 2 + c),
        dev(z, yp, tp), dev(z, ym, tp), dev(z, yo, tp), dev(zp, y, tp), dev(zm, y, tp),
    ]
    barrier = pltpu.get_barrier_semaphore()
    for other in near:
        pl.semaphore_signal(barrier, inc=1, device_id=other, device_id_type=MESH)
    pl.semaphore_wait(barrier, len(near))

    sent = []

    def rcopy(src, dst, ssem, rsem, to):
        return pltpu.make_async_remote_copy(
            src_ref=src, dst_ref=dst, send_sem=ssem, recv_sem=rsem, device_id=to, device_id_type=MESH
        )

    def send(*args):
        copy = rcopy(*args)
        copy.start()
        sent.append(copy)

    tokens = Exchange(xbuf, 2 * BLK, x, c, kv, a_s, a_r)
    loads[0].wait()
    tokens.own(0)
    tokens.own(1)
    send(req_in.at[yp], rbuf.at[2], rs.at[2], rr.at[2], dev(z, yp, tp))
    send(req_in.at[yo], rbuf.at[1], rs.at[1], rr.at[1], dev(z, yo, tp))
    send(req_in.at[ym], rbuf.at[0], rs.at[0], rr.at[0], dev(z, ym, tp))
    for load in loads[1:]:
        load.wait()

    def project(k):
        rows = pl.ds(k * 2 * BLK, 2 * BLK)
        total = None
        for t in range(8):
            term = jnp.dot(xbuf[t, rows, :], wqkv[t * COLS:(t + 1) * COLS, :], preferred_element_type=F32)
            total = term if total is None else total + term
        rounded = total.astype(BF)
        for i in range(2):
            b = 2 * k + i
            here = rounded[i * BLK:(i + 1) * BLK]
            own[b] = here[:, 256:512]
            pool[OWN + b] = here[:, 256:512]
            qs[b, 0:BLK, :] = here[:, 0:128]
            qs[b, BLK:2 * BLK, :] = here[:, 128:256]

    def piece(s):
        return pl.ds(2 * s, 2)

    def fwd(k, s):
        src = own if k == 1 else units_f[k - 2]
        return (src.at[piece(s)], units_f[k - 1].at[piece(s)], zs.at[0, k - 1, s], zr.at[0, k - 1, s], dev(zp, y, tp))

    def bwd(k, s):
        src = own if k == 1 else units_b[k - 2]
        return (src.at[piece(s)], units_b[k - 1].at[piece(s)], zs.at[1, k - 1, s], zr.at[1, k - 1, s], dev(zm, y, tp))

    def mid_fwd():
        return (units_f[6].at[pl.ds(0, 3)], mid.at[pl.ds(0, 3)], ms.at[0], mr.at[0], dev(zp, y, tp))

    def mid_bwd():
        return (units_b[6].at[pl.ds(3, 3)], mid.at[pl.ds(3, 3)], ms.at[1], mr.at[1], dev(zm, y, tp))

    def finish_chunk(k):
        tokens.finish(k)
        project(k)
        send(*fwd(1, k))
        send(*bwd(1, k))

    tokens.direct(0)
    tokens.own(2)
    tokens.direct(1)
    tokens.relayed(0)
    finish_chunk(0)
    tokens.direct(2)
    tokens.relayed(1)
    finish_chunk(1)
    tokens.relayed(2)
    finish_chunk(2)

    mine = pltpu.make_async_copy(req_in.at[y], req_sm.at[0], smem_sem.at[0])
    mine.start()
    asked = []
    for i in range(3):
        rcopy(rbuf.at[i], rbuf.at[i], rs.at[i], rr.at[i], dev(z, yp, tp)).wait_recv()
        asked.append(pltpu.make_async_copy(rbuf.at[i], req_sm.at[i + 1], smem_sem.at[i + 1]))
        asked[-1].start()
    mine.wait()
    for copy in asked:
        copy.wait()

    def up(d):
        return (stage.at[d, pl.ds(0, 3)], pool.at[pl.ds(d * PER + 2, 3)], ys.at[d, 0], yr.at[d, 0], dev(z, yp, tp))

    def down(d):
        return (stage.at[d, pl.ds(3, 3)], pool.at[pl.ds(d * PER + 5, 3)], ys.at[d, 1], yr.at[d, 1], dev(z, ym, tp))

    def far_up(d):
        return (pool.at[d * PER + 4], pool.at[d * PER + 8], os_.at[d, 0], or_.at[d, 0], dev(z, yp, tp))

    def far_down(d):
        return (pool.at[d * PER + 7], pool.at[d * PER + 9], os_.at[d, 1], or_.at[d, 1], dev(z, ym, tp))

    def pick(unit, d):
        hz = (z + NZ - d) % NZ

        def block(role, slot):
            return unit[req_sm[role, 0, hz * 2 + slot]]

        stage[d, 0] = block(1, 0)
        stage[d, 1] = block(1, 1)
        stage[d, 2] = block(2, 0)
        stage[d, 3] = block(3, 0)
        stage[d, 4] = block(3, 1)
        stage[d, 5] = block(2, 1)
        pool[d * PER] = block(0, 0)
        pool[d * PER + 1] = block(0, 1)
        send(*up(d))
        send(*down(d))

    def relay(d):
        rcopy(*up(d)).wait_recv()
        send(*far_up(d))
        rcopy(*down(d)).wait_recv()
        send(*far_down(d))

    pick(own, 0)
    waiting = [0]
    for k in range(1, 8):
        for s in range(3):
            rcopy(*fwd(k, s)).wait_recv()
            if k < 7:
                send(*fwd(k + 1, s))
            elif s == 1:
                send(*mid_fwd())
            rcopy(*bwd(k, s)).wait_recv()
            if k < 7:
                send(*bwd(k + 1, s))
            elif s == 2:
                send(*mid_bwd())
        pick(units_f[k - 1], k)
        pick(units_b[k - 1], NZ - k)
        for d in waiting:
            relay(d)
        waiting = [k, NZ - k]
    rcopy(*mid_fwd()).wait_recv()
    rcopy(*mid_bwd()).wait_recv()
    pick(mid, 8)
    for d in waiting:
        relay(d)
    relay(8)
    for d in range(NZ):
        rcopy(*far_up(d)).wait_recv()
        rcopy(*far_down(d)).wait_recv()

    heads = Exchange(hbuf, BLK, x, c, kv, e_s, e_r)
    row = lax.broadcasted_iota(jnp.int32, (2 * BLK, 128), 0) % BLK
    col = lax.broadcasted_iota(jnp.int32, (2 * BLK, 128), 1)
    late = (col < BLK) & (col > row)

    def attend(b):
        here = kvs.at[b % 2]
        for j in range(TOPB):
            here[j * BLK:(j + 1) * BLK, :] = pool[idx_ref[b, j]]
        scores = lax.dot_general(
            qs[b], here[:, 0:HD], (((1,), (1,)), ((), ())), preferred_element_type=F32
        ) + bias_ref[b:b + 1, :]
        scores = jnp.concatenate([jnp.where(late, -jnp.inf, scores[:, 0:128]), scores[:, 128:]], axis=1)
        peak = jnp.max(scores, axis=1, keepdims=True)
        weights = jnp.exp2((scores - peak) * EXP_SCALE)
        total = jnp.sum(weights, axis=1, keepdims=True)
        mixed = jnp.dot(weights.astype(BF), here[:, HD:2 * HD], preferred_element_type=F32) / total
        mixed = mixed.astype(BF)
        rows = pl.ds(b * BLK, BLK)
        hbuf[tp, rows, 0:HD] = mixed[0:BLK]
        hbuf[tp, rows, HD:2 * HD] = mixed[BLK:2 * BLK]

    def output(b):
        rows = pl.ds(b * BLK, BLK)
        total = None
        for t in range(8):
            term = jnp.dot(hbuf[t, rows, :], wos[t * COLS:(t + 1) * COLS, :], preferred_element_type=F32)
            total = term if total is None else total + term
        out_ref[rows, :] = total.astype(BF)

    for t in range(NB + 5):
        if t < NB:
            attend(t)
            heads.own(t)
        if 0 <= t - 2 < NB:
            heads.direct(t - 2)
        if 0 <= t - 4 < NB:
            heads.relayed(t - 4)
        if 0 <= t - 5 < NB:
            heads.finish(t - 5)
            output(t - 5)

    tokens.drain()
    heads.drain()
    for copy in sent:
        copy.wait_send()


def tables(chosen):
    device = lax.axis_index("kv")
    z, y = device // NY, device % NY
    holder = chosen // NB
    inner = chosen - holder * NB
    far_holder = holder[:, 4:].reshape(-1)
    far_inner = inner[:, 4:].reshape(-1)
    asked = far_holder[None, :] == jnp.arange(NZ * NY)[:, None]
    low = jnp.min(jnp.where(asked, far_inner[None, :], NB - 1), axis=1)
    high = jnp.max(jnp.where(asked, far_inner[None, :], 0), axis=1)
    both = jnp.stack([low, high], axis=1).reshape(NZ, NY, 2).transpose(1, 0, 2).reshape(NY, 1, 2 * NZ)
    req = jnp.broadcast_to(jnp.pad(both, ((0, 0), (0, 0), (0, 128 - 2 * NZ))), (NY, 8, 128))
    second = jnp.any(
        (far_holder[None, :] == far_holder[:, None]) & (far_inner[None, :] < far_inner[:, None]), axis=1
    ).astype(jnp.int32)
    second = jnp.pad(second.reshape(NB, TOPB - 4), ((0, 0), (4, 0)))
    step = (z - holder // NY) % NZ
    turn = (holder % NY - y) % NY
    place = jnp.where(turn == 0, 0, jnp.where(turn == 1, 5, jnp.where(turn == 2, 8, 2)))
    idx = jnp.where(holder == device, OWN + inner, step * PER + place + second)
    order = jnp.arange(TOPB)
    repeats = jnp.any(
        (chosen[:, :, None] == chosen[:, None, :]) & (order[None, None, :] < order[None, :, None]), axis=2
    )
    bias = jnp.where(repeats, -jnp.inf, 0.0).astype(F32)
    bias = jnp.broadcast_to(bias[:, :, None], (NB, TOPB, BLK)).reshape(NB, TOPB * BLK)
    return req.astype(jnp.int32), idx.astype(jnp.int32), bias


def local(tokens, query_weight, key_weight, value_weight, out_weight, chosen):
    req, idx, bias = tables(chosen)
    dma = pltpu.SemaphoreType.DMA
    hbm = pl.BlockSpec(memory_space=pl.ANY)
    vmem = pl.BlockSpec(memory_space=pltpu.VMEM)
    smem = pl.BlockSpec(memory_space=pltpu.SMEM)
    unit = pltpu.VMEM((NB, BLK, COLS), BF)
    scratch = [
        pltpu.VMEM((8, ROWS, COLS), BF),
        pltpu.VMEM((8, ROWS, COLS), BF),
        pltpu.VMEM((2048, 512), BF),
        pltpu.VMEM((2048, COLS), BF),
        pltpu.VMEM((NB, 2 * BLK, HD), BF),
        unit,
        unit,
        pltpu.VMEM((OWN + NB, BLK, COLS), BF),
        pltpu.VMEM((NZ, 6, BLK, COLS), BF),
        pltpu.VMEM((2, TOPB * BLK, COLS), BF),
        pltpu.VMEM((3, 8, 128), jnp.int32),
        pltpu.SMEM((4, 8, 128), jnp.int32),
        *([unit] * 14),
        dma((5,)),
        dma((3, 9)), dma((3, 9)),
        dma((NB, 9)), dma((NB, 9)),
        dma((2, 7, 3)), dma((2, 7, 3)),
        dma((2,)), dma((2,)),
        dma((NZ, 2)), dma((NZ, 2)),
        dma((NZ, 2)), dma((NZ, 2)),
        dma((3,)), dma((3,)),
        dma((4,)),
    ]
    return pl.pallas_call(
        kernel,
        out_shape=jax.ShapeDtypeStruct((ROWS, COLS), BF),
        in_specs=[hbm, hbm, hbm, hbm, hbm, vmem, smem, vmem],
        out_specs=vmem,
        scratch_shapes=scratch,
        compiler_params=pltpu.CompilerParams(
            collective_id=0, has_side_effects=True, vmem_limit_bytes=48 * 1024 * 1024
        ),
        name="layer",
    )(tokens, query_weight, key_weight, value_weight, out_weight, req, idx, bias)


def solution(mesh):
    placed = (P("kv", "tp"), P(None, "tp"), P(None, "tp"), P(None, "tp"), P(None, "tp"), P("kv", None))
    return jax.shard_map(local, mesh=mesh, in_specs=placed, out_specs=P("kv", "tp"), check_vma=False)
```

```python
import math

import jax
import jax.numpy as jnp
from jax import lax
from jax.experimental import pallas as pl
from jax.experimental.pallas import tpu as pltpu
from jax.sharding import PartitionSpec as P

HD = 128
BLK = 64
TOPB = 16
NB = 6
NX, NY, NZ = 4, 4, 16
ROWS = NB * BLK
COLS = 256
PER = 10
OWN = NZ * PER
MESH = pl.DeviceIdType.MESH
BF = jnp.bfloat16
F32 = jnp.float32
EXP_SCALE = HD ** (-0.5) * math.log2(math.e)


class Exchange:
    def __init__(self, buf, rows, x, c, kv, ssem, rsem):
        self.buf, self.rows, self.x, self.c, self.kv = buf, rows, x, c, kv
        self.ssem, self.rsem = ssem, rsem
        self.xp, self.xm, self.xo = (x + 1) % NX, (x + NX - 1) % NX, (x + 2) % NX
        self.pc = 1 - c
        self.sent = []

    def part(self, x, c, chunk, half=None):
        rows = self.rows if half is None else self.rows // 2
        start = chunk * self.rows + (0 if half is None else half * rows)
        return self.buf.at[x * 2 + c, pl.ds(start, rows), :]

    def copy(self, ref, chunk, kind, x, c):
        return pltpu.make_async_remote_copy(
            src_ref=ref, dst_ref=ref, send_sem=self.ssem.at[chunk, kind], recv_sem=self.rsem.at[chunk, kind],
            device_id={"kv": self.kv, "tp": x * 2 + c}, device_id_type=MESH,
        )

    def send(self, ref, chunk, kind, x, c):
        copy = self.copy(ref, chunk, kind, x, c)
        copy.start()
        self.sent.append(copy)

    def got(self, ref, chunk, kind):
        self.copy(ref, chunk, kind, self.x, self.pc).wait_recv()

    def own(self, k):
        ref = self.part(self.x, self.c, k)
        self.send(ref, k, 0, self.xp, self.c)
        self.send(ref, k, 1, self.xm, self.c)
        self.send(ref, k, 2, self.x, self.pc)

    def direct(self, k):
        self.got(self.part(self.xm, self.c, k), k, 0)
        self.send(self.part(self.xm, self.c, k, 0), k, 3, self.xp, self.c)
        self.send(self.part(self.xm, self.c, k), k, 5, self.x, self.pc)
        self.got(self.part(self.xp, self.c, k), k, 1)
        self.send(self.part(self.xp, self.c, k, 1), k, 4, self.xm, self.c)
        self.send(self.part(self.xp, self.c, k), k, 6, self.x, self.pc)

    def relayed(self, k):
        for half in (0, 1):
            ref = self.part(self.xo, self.c, k, half)
            self.got(ref, k, 3 + half)
            self.send(ref, k, 7 + half, self.x, self.pc)

    def finish(self, k):
        self.got(self.part(self.x, self.pc, k), k, 2)
        self.got(self.part(self.xm, self.pc, k), k, 5)
        self.got(self.part(self.xp, self.pc, k), k, 6)
        self.got(self.part(self.xo, self.pc, k, 0), k, 7)
        self.got(self.part(self.xo, self.pc, k, 1), k, 8)

    def drain(self):
        for copy in self.sent:
            copy.wait_send()


def kernel(tok, wq, wk, wv, wo, req_in, idx_ref, bias_ref, out_ref, *scratch):
    (xbuf, hbuf, wqkv, wos, qs, own, mid, pool, stage, kvs, rbuf, req_sm) = scratch[:12]
    units_f, units_b = scratch[12:19], scratch[19:26]
    (lsem, a_s, a_r, e_s, e_r, zs, zr, ms, mr, ys, yr, os_, or_, rs, rr, smem_sem) = scratch[26:]

    kv = lax.axis_index("kv")
    tp = lax.axis_index("tp")
    z, y = kv // NY, kv % NY
    x, c = tp // 2, tp % 2
    yp, ym, yo = (y + 1) % NY, (y + NY - 1) % NY, (y + 2) % NY
    zp, zm = (z + 1) % NZ, (z + NZ - 1) % NZ

    loads = [
        pltpu.make_async_copy(tok, xbuf.at[tp], lsem.at[0]),
        pltpu.make_async_copy(wq, wqkv.at[:, 0:256], lsem.at[1]),
        pltpu.make_async_copy(wk, wqkv.at[:, 256:384], lsem.at[2]),
        pltpu.make_async_copy(wv, wqkv.at[:, 384:512], lsem.at[3]),
        pltpu.make_async_copy(wo, wos, lsem.at[4]),
    ]
    for load in loads:
        load.start()

    def dev(zz, yy, tt):
        return {"kv": zz * NY + yy, "tp": tt}

    near = [
        dev(z, y, x * 2 + 1 - c), dev(z, y, ((x + 1) % NX) * 2 + c), dev(z, y, ((x + 3) % NX) * 2 + c),
        dev(z, yp, tp), dev(z, ym, tp), dev(z, yo, tp), dev(zp, y, tp), dev(zm, y, tp),
    ]
    barrier = pltpu.get_barrier_semaphore()
    for other in near:
        pl.semaphore_signal(barrier, inc=1, device_id=other, device_id_type=MESH)
    pl.semaphore_wait(barrier, len(near))

    sent = []

    def rcopy(src, dst, ssem, rsem, to):
        return pltpu.make_async_remote_copy(
            src_ref=src, dst_ref=dst, send_sem=ssem, recv_sem=rsem, device_id=to, device_id_type=MESH
        )

    def send(*args, only=None):
        copy = rcopy(*args)
        if only is None:
            copy.start()
        else:
            pl.when(only)(copy.start)
        sent.append((only, copy))

    def wait(*args, only):
        pl.when(only)(rcopy(*args).wait_recv)

    tokens = Exchange(xbuf, 2 * BLK, x, c, kv, a_s, a_r)
    loads[0].wait()
    tokens.own(0)
    tokens.own(1)
    send(req_in.at[yp], rbuf.at[2], rs.at[2], rr.at[2], dev(z, yp, tp))
    send(req_in.at[yo], rbuf.at[1], rs.at[1], rr.at[1], dev(z, yo, tp))
    send(req_in.at[ym], rbuf.at[0], rs.at[0], rr.at[0], dev(z, ym, tp))
    for load in loads[1:]:
        load.wait()

    def project(k):
        rows = pl.ds(k * 2 * BLK, 2 * BLK)
        total = None
        for t in range(8):
            term = jnp.dot(xbuf[t, rows, :], wqkv[t * COLS:(t + 1) * COLS, :], preferred_element_type=F32)
            total = term if total is None else total + term
        rounded = total.astype(BF)
        for i in range(2):
            b = 2 * k + i
            here = rounded[i * BLK:(i + 1) * BLK]
            own[b] = here[:, 256:512]
            pool[OWN + b] = here[:, 256:512]
            qs[b, 0:BLK, :] = here[:, 0:128]
            qs[b, BLK:2 * BLK, :] = here[:, 128:256]

    def goes_up(k):
        return (z >= k - 1) & (z < NZ - 1)

    def comes_up(k):
        return z >= k

    def goes_down(k):
        return (z + k - 1) % NZ <= 7

    def comes_down(k):
        return (z + k) % NZ <= 7

    def piece(s):
        return pl.ds(2 * s, 2)

    def fwd(k, s):
        src = own if k == 1 else units_f[k - 2]
        return (src.at[piece(s)], units_f[k - 1].at[piece(s)], zs.at[0, k - 1, s], zr.at[0, k - 1, s], dev(zp, y, tp))

    def bwd(k, s):
        src = own if k == 1 else units_b[k - 2]
        return (src.at[piece(s)], units_b[k - 1].at[piece(s)], zs.at[1, k - 1, s], zr.at[1, k - 1, s], dev(zm, y, tp))

    def mid_fwd():
        return (units_f[6].at[pl.ds(0, 3)], mid.at[pl.ds(0, 3)], ms.at[0], mr.at[0], dev(zp, y, tp))

    def mid_bwd():
        return (units_b[6].at[pl.ds(3, 3)], mid.at[pl.ds(3, 3)], ms.at[1], mr.at[1], dev(zm, y, tp))

    def finish_chunk(k):
        tokens.finish(k)
        project(k)
        send(*fwd(1, k), only=goes_up(1))
        send(*bwd(1, k), only=goes_down(1))

    tokens.direct(0)
    tokens.own(2)
    tokens.direct(1)
    tokens.relayed(0)
    finish_chunk(0)
    tokens.direct(2)
    tokens.relayed(1)
    finish_chunk(1)
    tokens.relayed(2)
    finish_chunk(2)

    mine = pltpu.make_async_copy(req_in.at[y], req_sm.at[0], smem_sem.at[0])
    mine.start()
    asked = []
    for i in range(3):
        rcopy(rbuf.at[i], rbuf.at[i], rs.at[i], rr.at[i], dev(z, yp, tp)).wait_recv()
        asked.append(pltpu.make_async_copy(rbuf.at[i], req_sm.at[i + 1], smem_sem.at[i + 1]))
        asked[-1].start()
    mine.wait()
    for copy in asked:
        copy.wait()

    def up(d):
        return (stage.at[d, pl.ds(0, 3)], pool.at[pl.ds(d * PER + 2, 3)], ys.at[d, 0], yr.at[d, 0], dev(z, yp, tp))

    def down(d):
        return (stage.at[d, pl.ds(3, 3)], pool.at[pl.ds(d * PER + 5, 3)], ys.at[d, 1], yr.at[d, 1], dev(z, ym, tp))

    def far_up(d):
        return (pool.at[d * PER + 4], pool.at[d * PER + 8], os_.at[d, 0], or_.at[d, 0], dev(z, yp, tp))

    def far_down(d):
        return (pool.at[d * PER + 7], pool.at[d * PER + 9], os_.at[d, 1], or_.at[d, 1], dev(z, ym, tp))

    def pick(unit, d):
        hz = (z + NZ - d) % NZ

        def block(role, slot):
            return unit[req_sm[role, 0, hz * 2 + slot]]

        @pl.when(z >= d)
        def _():
            stage[d, 0] = block(1, 0)
            stage[d, 1] = block(1, 1)
            stage[d, 2] = block(2, 0)
            stage[d, 3] = block(3, 0)
            stage[d, 4] = block(3, 1)
            stage[d, 5] = block(2, 1)
            pool[d * PER] = block(0, 0)
            pool[d * PER + 1] = block(0, 1)

        send(*up(d), only=z >= d)
        send(*down(d), only=z >= d)

    def relay(d):
        wait(*up(d), only=z >= d)
        send(*far_up(d), only=z >= d)
        wait(*down(d), only=z >= d)
        send(*far_down(d), only=z >= d)

    pick(own, 0)
    waiting = [0]
    for k in range(1, 8):
        for s in range(3):
            wait(*fwd(k, s), only=comes_up(k))
            if k < 7:
                send(*fwd(k + 1, s), only=goes_up(k + 1))
            elif s == 1:
                send(*mid_fwd(), only=goes_up(8))
            wait(*bwd(k, s), only=comes_down(k))
            if k < 7:
                send(*bwd(k + 1, s), only=goes_down(k + 1))
            elif s == 2:
                send(*mid_bwd(), only=goes_down(8))
        pick(units_f[k - 1], k)
        pick(units_b[k - 1], NZ - k)
        for d in waiting:
            relay(d)
        waiting = [k, NZ - k]
    wait(*mid_fwd(), only=comes_up(8))
    wait(*mid_bwd(), only=comes_down(8))
    pick(mid, 8)
    for d in waiting:
        relay(d)
    relay(8)
    for d in range(NZ):
        wait(*far_up(d), only=z >= d)
        wait(*far_down(d), only=z >= d)

    heads = Exchange(hbuf, BLK, x, c, kv, e_s, e_r)
    row = lax.broadcasted_iota(jnp.int32, (2 * BLK, 128), 0) % BLK
    col = lax.broadcasted_iota(jnp.int32, (2 * BLK, 128), 1)
    late = (col < BLK) & (col > row)

    def attend(b):
        here = kvs.at[b % 2]
        for j in range(TOPB):
            here[j * BLK:(j + 1) * BLK, :] = pool[idx_ref[b, j]]
        scores = lax.dot_general(
            qs[b], here[:, 0:HD], (((1,), (1,)), ((), ())), preferred_element_type=F32
        ) + bias_ref[b:b + 1, :]
        scores = jnp.concatenate([jnp.where(late, -jnp.inf, scores[:, 0:128]), scores[:, 128:]], axis=1)
        peak = jnp.max(scores, axis=1, keepdims=True)
        weights = jnp.exp2((scores - peak) * EXP_SCALE)
        total = jnp.sum(weights, axis=1, keepdims=True)
        mixed = jnp.dot(weights.astype(BF), here[:, HD:2 * HD], preferred_element_type=F32) / total
        mixed = mixed.astype(BF)
        rows = pl.ds(b * BLK, BLK)
        hbuf[tp, rows, 0:HD] = mixed[0:BLK]
        hbuf[tp, rows, HD:2 * HD] = mixed[BLK:2 * BLK]

    def output(b):
        rows = pl.ds(b * BLK, BLK)
        total = None
        for t in range(8):
            term = jnp.dot(hbuf[t, rows, :], wos[t * COLS:(t + 1) * COLS, :], preferred_element_type=F32)
            total = term if total is None else total + term
        out_ref[rows, :] = total.astype(BF)

    for b in range(NB):
        attend(b)
        heads.own(b)
    for b in range(NB):
        heads.direct(b)
    for b in range(NB + 1):
        if b < NB:
            heads.relayed(b)
        if b > 0:
            heads.finish(b - 1)
            output(b - 1)

    tokens.drain()
    heads.drain()
    for only, copy in sent:
        if only is None:
            copy.wait_send()
        else:
            pl.when(only)(copy.wait_send)


def tables(chosen):
    device = lax.axis_index("kv")
    z, y = device // NY, device % NY
    holder = chosen // NB
    inner = chosen - holder * NB
    far_holder = holder[:, 4:].reshape(-1)
    far_inner = inner[:, 4:].reshape(-1)
    asked = far_holder[None, :] == jnp.arange(NZ * NY)[:, None]
    low = jnp.min(jnp.where(asked, far_inner[None, :], NB - 1), axis=1)
    high = jnp.max(jnp.where(asked, far_inner[None, :], 0), axis=1)
    both = jnp.stack([low, high], axis=1).reshape(NZ, NY, 2).transpose(1, 0, 2).reshape(NY, 1, 2 * NZ)
    req = jnp.broadcast_to(jnp.pad(both, ((0, 0), (0, 0), (0, 128 - 2 * NZ))), (NY, 8, 128))
    second = jnp.any(
        (far_holder[None, :] == far_holder[:, None]) & (far_inner[None, :] < far_inner[:, None]), axis=1
    ).astype(jnp.int32)
    second = jnp.pad(second.reshape(NB, TOPB - 4), ((0, 0), (4, 0)))
    step = (z - holder // NY) % NZ
    turn = (holder % NY - y) % NY
    place = jnp.where(turn == 0, 0, jnp.where(turn == 1, 5, jnp.where(turn == 2, 8, 2)))
    idx = jnp.where(holder == device, OWN + inner, step * PER + place + second)
    order = jnp.arange(TOPB)
    repeats = jnp.any(
        (chosen[:, :, None] == chosen[:, None, :]) & (order[None, None, :] < order[None, :, None]), axis=2
    )
    bias = jnp.where(repeats, -jnp.inf, 0.0).astype(F32)
    bias = jnp.broadcast_to(bias[:, :, None], (NB, TOPB, BLK)).reshape(NB, TOPB * BLK)
    return req.astype(jnp.int32), idx.astype(jnp.int32), bias


def local(tokens, query_weight, key_weight, value_weight, out_weight, chosen):
    req, idx, bias = tables(chosen)
    dma = pltpu.SemaphoreType.DMA
    hbm = pl.BlockSpec(memory_space=pl.ANY)
    vmem = pl.BlockSpec(memory_space=pltpu.VMEM)
    smem = pl.BlockSpec(memory_space=pltpu.SMEM)
    unit = pltpu.VMEM((NB, BLK, COLS), BF)
    scratch = [
        pltpu.VMEM((8, ROWS, COLS), BF),
        pltpu.VMEM((8, ROWS, COLS), BF),
        pltpu.VMEM((2048, 512), BF),
        pltpu.VMEM((2048, COLS), BF),
        pltpu.VMEM((NB, 2 * BLK, HD), BF),
        unit,
        unit,
        pltpu.VMEM((OWN + NB, BLK, COLS), BF),
        pltpu.VMEM((NZ, 6, BLK, COLS), BF),
        pltpu.VMEM((2, TOPB * BLK, COLS), BF),
        pltpu.VMEM((3, 8, 128), jnp.int32),
        pltpu.SMEM((4, 8, 128), jnp.int32),
        *([unit] * 14),
        dma((5,)),
        dma((3, 9)), dma((3, 9)),
        dma((NB, 9)), dma((NB, 9)),
        dma((2, 7, 3)), dma((2, 7, 3)),
        dma((2,)), dma((2,)),
        dma((NZ, 2)), dma((NZ, 2)),
        dma((NZ, 2)), dma((NZ, 2)),
        dma((3,)), dma((3,)),
        dma((4,)),
    ]
    return pl.pallas_call(
        kernel,
        out_shape=jax.ShapeDtypeStruct((ROWS, COLS), BF),
        in_specs=[hbm, hbm, hbm, hbm, hbm, vmem, smem, vmem],
        out_specs=vmem,
        scratch_shapes=scratch,
        compiler_params=pltpu.CompilerParams(
            collective_id=0, has_side_effects=True, vmem_limit_bytes=62 * 1024 * 1024
        ),
        name="layer",
    )(tokens, query_weight, key_weight, value_weight, out_weight, req, idx, bias)


def solution(mesh):
    placed = (P("kv", "tp"), P(None, "tp"), P(None, "tp"), P(None, "tp"), P(None, "tp"), P("kv", None))
    return jax.shard_map(local, mesh=mesh, in_specs=placed, out_specs=P("kv", "tp"), check_vma=False)
```

```python
import math

import jax
import jax.numpy as jnp
from jax import lax
from jax.experimental import pallas as pl
from jax.experimental.pallas import tpu as pltpu
from jax.sharding import PartitionSpec as P

HD = 128
BLK = 64
TOPB = 16
NB = 6
NX, NY, NZ = 4, 4, 16
ROWS = NB * BLK
COLS = 256
PER = 6
FAR = 4
OWN = NZ * PER
FLOOR = -1e30
MESH = pl.DeviceIdType.MESH
BF = jnp.bfloat16
F32 = jnp.float32
EXP_SCALE = HD ** (-0.5) * math.log2(math.e)


class Exchange:
    def __init__(self, buf, rows, x, c, kv, ssem, rsem):
        self.buf, self.rows, self.x, self.c, self.kv = buf, rows, x, c, kv
        self.ssem, self.rsem = ssem, rsem
        self.xp, self.xm, self.xo = (x + 1) % NX, (x + NX - 1) % NX, (x + 2) % NX
        self.pc = 1 - c
        self.sent = []

    def part(self, x, c, chunk, half=None):
        rows = self.rows if half is None else self.rows // 2
        start = chunk * self.rows + (0 if half is None else half * rows)
        return self.buf.at[x * 2 + c, pl.ds(start, rows), :]

    def copy(self, ref, chunk, kind, x, c):
        return pltpu.make_async_remote_copy(
            src_ref=ref, dst_ref=ref, send_sem=self.ssem.at[chunk, kind], recv_sem=self.rsem.at[chunk, kind],
            device_id={"kv": self.kv, "tp": x * 2 + c}, device_id_type=MESH,
        )

    def send(self, ref, chunk, kind, x, c):
        copy = self.copy(ref, chunk, kind, x, c)
        copy.start()
        self.sent.append(copy)

    def got(self, ref, chunk, kind):
        self.copy(ref, chunk, kind, self.x, self.pc).wait_recv()

    def own(self, k):
        ref = self.part(self.x, self.c, k)
        self.send(ref, k, 0, self.xp, self.c)
        self.send(ref, k, 1, self.xm, self.c)
        self.send(ref, k, 2, self.x, self.pc)

    def direct(self, k):
        self.got(self.part(self.xm, self.c, k), k, 0)
        self.send(self.part(self.xm, self.c, k, 0), k, 3, self.xp, self.c)
        self.send(self.part(self.xm, self.c, k), k, 5, self.x, self.pc)
        self.got(self.part(self.xp, self.c, k), k, 1)
        self.send(self.part(self.xp, self.c, k, 1), k, 4, self.xm, self.c)
        self.send(self.part(self.xp, self.c, k), k, 6, self.x, self.pc)

    def relayed(self, k):
        for half in (0, 1):
            ref = self.part(self.xo, self.c, k, half)
            self.got(ref, k, 3 + half)
            self.send(ref, k, 7 + half, self.x, self.pc)

    def finish(self, k):
        self.got(self.part(self.x, self.pc, k), k, 2)
        self.got(self.part(self.xm, self.pc, k), k, 5)
        self.got(self.part(self.xp, self.pc, k), k, 6)
        self.got(self.part(self.xo, self.pc, k, 0), k, 7)
        self.got(self.part(self.xo, self.pc, k, 1), k, 8)

    def drain(self):
        for copy in self.sent:
            copy.wait_send()


def kernel(tok, wq, wk, wv, wo, req_in, idx_ref, bias_ref, far_bias, out_ref, *scratch):
    (xbuf, hbuf, wqkv, wos, qs, own, mid, pool, stage, kvs, rbuf, req_sm) = scratch[:12]
    units_f, units_b = scratch[12:19], scratch[19:26]
    (fpool, fkvs, qin, qrel, fbias, ret, lse, back_rel, back, back_lse, acc, mass) = scratch[26:38]
    (lsem, a_s, a_r, e_s, e_r, zs, zr, ms, mr, ys, yr, rs, rr, smem_sem, q1s, q1r, q2s, q2r, bs, br, b1s, b1r, b2s, b2r,
     ls, lr) = scratch[38:]

    kv = lax.axis_index("kv")
    tp = lax.axis_index("tp")
    z, y = kv // NY, kv % NY
    x, c = tp // 2, tp % 2
    yp, ym, yo = (y + 1) % NY, (y + NY - 1) % NY, (y + 2) % NY
    zp, zm = (z + 1) % NZ, (z + NZ - 1) % NZ

    loads = [
        pltpu.make_async_copy(tok, xbuf.at[tp], lsem.at[0]),
        pltpu.make_async_copy(wq, wqkv.at[:, 0:256], lsem.at[1]),
        pltpu.make_async_copy(wk, wqkv.at[:, 256:384], lsem.at[2]),
        pltpu.make_async_copy(wv, wqkv.at[:, 384:512], lsem.at[3]),
        pltpu.make_async_copy(wo, wos, lsem.at[4]),
    ]
    for load in loads:
        load.start()

    def dev(zz, yy, tt):
        return {"kv": zz * NY + yy, "tp": tt}

    near = [
        dev(z, y, x * 2 + 1 - c), dev(z, y, ((x + 1) % NX) * 2 + c), dev(z, y, ((x + 3) % NX) * 2 + c),
        dev(z, yp, tp), dev(z, ym, tp), dev(z, yo, tp), dev(zp, y, tp), dev(zm, y, tp),
    ]
    barrier = pltpu.get_barrier_semaphore()
    for other in near:
        pl.semaphore_signal(barrier, inc=1, device_id=other, device_id_type=MESH)
    pl.semaphore_wait(barrier, len(near))

    sent = []

    def rcopy(src, dst, ssem, rsem, to):
        return pltpu.make_async_remote_copy(
            src_ref=src, dst_ref=dst, send_sem=ssem, recv_sem=rsem, device_id=to, device_id_type=MESH
        )

    def send(*args, only=None):
        copy = rcopy(*args)
        if only is None:
            copy.start()
        else:
            pl.when(only)(copy.start)
        sent.append((only, copy))

    def wait(*args, only):
        pl.when(only)(rcopy(*args).wait_recv)

    tokens = Exchange(xbuf, 2 * BLK, x, c, kv, a_s, a_r)
    loads[0].wait()
    tokens.own(0)
    tokens.own(1)
    send(req_in.at[yp], rbuf.at[2], rs.at[2], rr.at[2], dev(z, yp, tp))
    send(req_in.at[yo], rbuf.at[1], rs.at[1], rr.at[1], dev(z, yo, tp))
    send(req_in.at[ym], rbuf.at[0], rs.at[0], rr.at[0], dev(z, ym, tp))
    send(far_bias, fbias, bs.at[0], br.at[0], dev(z, yo, tp))
    for load in loads[1:]:
        load.wait()

    def project(k):
        rows = pl.ds(k * 2 * BLK, 2 * BLK)
        total = None
        for t in range(8):
            term = jnp.dot(xbuf[t, rows, :], wqkv[t * COLS:(t + 1) * COLS, :], preferred_element_type=F32)
            total = term if total is None else total + term
        rounded = total.astype(BF)
        for i in range(2):
            b = 2 * k + i
            here = rounded[i * BLK:(i + 1) * BLK]
            own[b] = here[:, 256:512]
            pool[OWN + b] = here[:, 256:512]
            qs[b, 0:BLK, :] = here[:, 0:128]
            qs[b, BLK:2 * BLK, :] = here[:, 128:256]

    def goes_up(k):
        return (z >= k - 1) & (z < NZ - 1)

    def comes_up(k):
        return z >= k

    def goes_down(k):
        return (z + k - 1) % NZ <= 7

    def comes_down(k):
        return (z + k) % NZ <= 7

    def piece(s):
        return pl.ds(2 * s, 2)

    def fwd(k, s):
        src = own if k == 1 else units_f[k - 2]
        return (src.at[piece(s)], units_f[k - 1].at[piece(s)], zs.at[0, k - 1, s], zr.at[0, k - 1, s], dev(zp, y, tp))

    def bwd(k, s):
        src = own if k == 1 else units_b[k - 2]
        return (src.at[piece(s)], units_b[k - 1].at[piece(s)], zs.at[1, k - 1, s], zr.at[1, k - 1, s], dev(zm, y, tp))

    def mid_fwd():
        return (units_f[6].at[pl.ds(0, 3)], mid.at[pl.ds(0, 3)], ms.at[0], mr.at[0], dev(zp, y, tp))

    def mid_bwd():
        return (units_b[6].at[pl.ds(3, 3)], mid.at[pl.ds(3, 3)], ms.at[1], mr.at[1], dev(zm, y, tp))

    def finish_chunk(k):
        tokens.finish(k)
        project(k)
        send(*fwd(1, k), only=goes_up(1))
        send(*bwd(1, k), only=goes_down(1))

    tokens.direct(0)
    tokens.own(2)
    tokens.direct(1)
    tokens.relayed(0)
    finish_chunk(0)
    tokens.direct(2)
    tokens.relayed(1)
    finish_chunk(1)
    tokens.relayed(2)
    finish_chunk(2)

    def ship(i):
        to = dev(z, yp, tp) if i == 0 else dev(z, ym, tp)
        return (qs.at[pl.ds(3 * i, 3)], qrel.at[i], q1s.at[i], q1r.at[i], to)

    def ship_on(i):
        to = dev(z, yp, tp) if i == 0 else dev(z, ym, tp)
        return (qrel.at[i], qin.at[pl.ds(3 * i, 3)], q2s.at[i], q2r.at[i], to)

    send(*ship(0))
    send(*ship(1))

    mine = pltpu.make_async_copy(req_in.at[y], req_sm.at[0], smem_sem.at[0])
    mine.start()
    asked = []
    for i in range(3):
        rcopy(rbuf.at[i], rbuf.at[i], rs.at[i], rr.at[i], dev(z, yp, tp)).wait_recv()
        asked.append(pltpu.make_async_copy(rbuf.at[i], req_sm.at[i + 1], smem_sem.at[i + 1]))
        asked[-1].start()
    mine.wait()
    for copy in asked:
        copy.wait()

    def up(d):
        return (stage.at[d, pl.ds(0, 2)], pool.at[pl.ds(d * PER + 2, 2)], ys.at[d, 0], yr.at[d, 0], dev(z, yp, tp))

    def down(d):
        return (stage.at[d, pl.ds(2, 2)], pool.at[pl.ds(d * PER + 4, 2)], ys.at[d, 1], yr.at[d, 1], dev(z, ym, tp))

    def pick(unit, d):
        hz = (z + NZ - d) % NZ

        def block(role, slot):
            return unit[req_sm[role, 0, hz * 2 + slot]]

        @pl.when(z >= d)
        def _():
            stage[d, 0] = block(1, 0)
            stage[d, 1] = block(1, 1)
            stage[d, 2] = block(3, 0)
            stage[d, 3] = block(3, 1)
            fpool[2 * d] = block(2, 0)
            fpool[2 * d + 1] = block(2, 1)
            pool[d * PER] = block(0, 0)
            pool[d * PER + 1] = block(0, 1)

        send(*up(d), only=z >= d)
        send(*down(d), only=z >= d)

    pick(own, 0)
    for k in range(1, 8):
        for s in range(3):
            wait(*fwd(k, s), only=comes_up(k))
            if k < 7:
                send(*fwd(k + 1, s), only=goes_up(k + 1))
            elif s == 1:
                send(*mid_fwd(), only=goes_up(8))
            wait(*bwd(k, s), only=comes_down(k))
            if k < 7:
                send(*bwd(k + 1, s), only=goes_down(k + 1))
            elif s == 2:
                send(*mid_bwd(), only=goes_down(8))
        pick(units_f[k - 1], k)
        pick(units_b[k - 1], NZ - k)
        if k == 2:
            for i in range(2):
                rcopy(*ship(i)).wait_recv()
                send(*ship_on(i))
    wait(*mid_fwd(), only=comes_up(8))
    wait(*mid_bwd(), only=comes_down(8))
    pick(mid, 8)
    heads = Exchange(hbuf, BLK, x, c, kv, e_s, e_r)
    row = lax.broadcasted_iota(jnp.int32, (2 * BLK, 128), 0) % BLK
    col = lax.broadcasted_iota(jnp.int32, (2 * BLK, 128), 1)
    late = (col < BLK) & (col > row)

    def back_first(b):
        to = dev(z, yp, tp) if b % 2 == 0 else dev(z, ym, tp)
        return (ret.at[b], back_rel.at[b], b1s.at[b], b1r.at[b], to)

    def back_on(b):
        to = dev(z, yp, tp) if b % 2 == 0 else dev(z, ym, tp)
        return (back_rel.at[b], back.at[b], b2s.at[b], b2r.at[b], to)

    def back_mass(b):
        return (lse.at[b], back_lse.at[b], ls.at[b], lr.at[b], dev(z, yo, tp))

    def attend_far(b):
        here = fkvs.at[b % 2]
        for j in range(FAR, TOPB):
            here[(j - FAR) * BLK:(j - FAR + 1) * BLK, :] = fpool[req_sm[2, 1, b * TOPB + j]]
        scores = lax.dot_general(
            qin[b], here[:, 0:HD], (((1,), (1,)), ((), ())), preferred_element_type=F32
        ) + fbias[b:b + 1, FAR * BLK:]
        peak = jnp.maximum(jnp.max(scores, axis=1, keepdims=True), FLOOR)
        weights = jnp.exp2((scores - peak) * EXP_SCALE)
        total = jnp.maximum(jnp.sum(weights, axis=1, keepdims=True), 1e-30)
        part = jnp.dot(weights.astype(BF), here[:, HD:2 * HD], preferred_element_type=F32) / total
        ret[b] = part.astype(BF)
        size = peak * EXP_SCALE + jnp.log(total) * math.log2(math.e)
        lse[b] = jnp.transpose(jnp.broadcast_to(size, (2 * BLK, 128)))[0:8]
        send(*back_first(b))
        send(*back_mass(b))

    def pass_back(b):
        rcopy(*back_first(b)).wait_recv()
        send(*back_on(b))

    def attend(b):
        here = kvs.at[b % 2]
        for j in range(TOPB):
            here[j * BLK:(j + 1) * BLK, :] = pool[idx_ref[b, j]]
        scores = lax.dot_general(
            qs[b], here[:, 0:HD], (((1,), (1,)), ((), ())), preferred_element_type=F32
        ) + bias_ref[b:b + 1, :]
        scores = jnp.concatenate([jnp.where(late, -jnp.inf, scores[:, 0:128]), scores[:, 128:]], axis=1)
        peak = jnp.max(scores, axis=1, keepdims=True)
        weights = jnp.exp2((scores - peak) * EXP_SCALE)
        acc[b] = jnp.dot(weights.astype(BF), here[:, HD:2 * HD], preferred_element_type=F32)
        mass[b, 0] = jnp.broadcast_to(peak * EXP_SCALE, (2 * BLK, 128))
        mass[b, 1] = jnp.broadcast_to(jnp.sum(weights, axis=1, keepdims=True), (2 * BLK, 128))

    def merge(b):
        rcopy(*back_on(b)).wait_recv()
        rcopy(*back_mass(b)).wait_recv()
        size = jnp.transpose(jnp.broadcast_to(back_lse[b, 0:1, :], (128, 2 * BLK)))
        peak = mass[b, 0]
        top = jnp.maximum(peak, size)
        mine, theirs = jnp.exp2(peak - top), jnp.exp2(size - top)
        mixed = (acc[b] * mine + back[b].astype(F32) * theirs) / (mass[b, 1] * mine + theirs)
        mixed = mixed.astype(BF)
        rows = pl.ds(b * BLK, BLK)
        hbuf[tp, rows, 0:HD] = mixed[0:BLK]
        hbuf[tp, rows, HD:2 * HD] = mixed[BLK:2 * BLK]

    def output(b):
        rows = pl.ds(b * BLK, BLK)
        total = None
        for t in range(8):
            term = jnp.dot(hbuf[t, rows, :], wos[t * COLS:(t + 1) * COLS, :], preferred_element_type=F32)
            total = term if total is None else total + term
        out_ref[rows, :] = total.astype(BF)

    for i in range(2):
        rcopy(*ship_on(i)).wait_recv()
    rcopy(far_bias, fbias, bs.at[0], br.at[0], dev(z, yo, tp)).wait_recv()
    for b in range(NB):
        attend_far(b)
    for d in range(NZ):
        wait(*up(d), only=z >= d)
        wait(*down(d), only=z >= d)
    attend(0)
    attend(1)
    pass_back(0)
    pass_back(1)
    for b in range(2, NB):
        attend(b)
        pass_back(b)
    for b in range(NB):
        merge(b)
        heads.own(b)
    for b in range(NB):
        heads.direct(b)
    for b in range(NB + 1):
        if b < NB:
            heads.relayed(b)
        if b > 0:
            heads.finish(b - 1)
            output(b - 1)

    tokens.drain()
    heads.drain()
    for only, copy in sent:
        if only is None:
            copy.wait_send()
        else:
            pl.when(only)(copy.wait_send)


def tables(chosen):
    device = lax.axis_index("kv")
    z, y = device // NY, device % NY
    holder = chosen // NB
    inner = chosen - holder * NB
    far_holder = holder[:, 4:].reshape(-1)
    far_inner = inner[:, 4:].reshape(-1)
    asked = far_holder[None, :] == jnp.arange(NZ * NY)[:, None]
    low = jnp.min(jnp.where(asked, far_inner[None, :], NB - 1), axis=1)
    high = jnp.max(jnp.where(asked, far_inner[None, :], 0), axis=1)
    both = jnp.stack([low, high], axis=1).reshape(NZ, NY, 2).transpose(1, 0, 2).reshape(NY, 1, 2 * NZ)
    second = jnp.any(
        (far_holder[None, :] == far_holder[:, None]) & (far_inner[None, :] < far_inner[:, None]), axis=1
    ).astype(jnp.int32)
    second = jnp.pad(second.reshape(NB, TOPB - 4), ((0, 0), (4, 0)))
    step = (z - holder // NY) % NZ
    turn = (holder % NY - y) % NY
    far = turn == 2
    place = jnp.where(turn == 0, 0, jnp.where(turn == 1, 4, 2))
    idx = jnp.where(holder == device, OWN + inner, jnp.where(far, OWN, step * PER + place + second))
    far_idx = jnp.where(far, 2 * step + second, 0).reshape(1, 1, NB * TOPB)
    far_row = jnp.broadcast_to(jnp.pad(far_idx, ((0, 0), (0, 0), (0, 128 - NB * TOPB))), (NY, 1, 128))
    req_row = jnp.pad(both, ((0, 0), (0, 0), (0, 128 - 2 * NZ)))
    req = jnp.concatenate([req_row, far_row, jnp.zeros((NY, 6, 128), jnp.int32)], axis=1)
    order = jnp.arange(TOPB)
    repeats = jnp.any(
        (chosen[:, :, None] == chosen[:, None, :]) & (order[None, None, :] < order[None, :, None]), axis=2
    )
    near_bias = jnp.where(repeats | far, -jnp.inf, 0.0).astype(F32)
    far_bias = jnp.where(far & ~repeats, 0.0, -jnp.inf).astype(F32)

    def spread(rows):
        return jnp.broadcast_to(rows[:, :, None], (NB, TOPB, BLK)).reshape(NB, TOPB * BLK)

    far_bias = jnp.pad(spread(far_bias), ((0, 2), (0, 0)))
    return req.astype(jnp.int32), idx.astype(jnp.int32), spread(near_bias), far_bias


def local(tokens, query_weight, key_weight, value_weight, out_weight, chosen):
    req, idx, bias, far_bias = tables(chosen)
    dma = pltpu.SemaphoreType.DMA
    hbm = pl.BlockSpec(memory_space=pl.ANY)
    vmem = pl.BlockSpec(memory_space=pltpu.VMEM)
    smem = pl.BlockSpec(memory_space=pltpu.SMEM)
    unit = pltpu.VMEM((NB, BLK, COLS), BF)
    scratch = [
        pltpu.VMEM((8, ROWS, COLS), BF),
        pltpu.VMEM((8, ROWS, COLS), BF),
        pltpu.VMEM((2048, 512), BF),
        pltpu.VMEM((2048, COLS), BF),
        pltpu.VMEM((NB, 2 * BLK, HD), BF),
        unit,
        unit,
        pltpu.VMEM((OWN + NB, BLK, COLS), BF),
        pltpu.VMEM((NZ, 4, BLK, COLS), BF),
        pltpu.VMEM((2, TOPB * BLK, COLS), BF),
        pltpu.VMEM((3, 8, 128), jnp.int32),
        pltpu.SMEM((4, 8, 128), jnp.int32),
        *([unit] * 14),
        pltpu.VMEM((2 * NZ, BLK, COLS), BF),
        pltpu.VMEM((2, (TOPB - FAR) * BLK, COLS), BF),
        pltpu.VMEM((NB, 2 * BLK, HD), BF),
        pltpu.VMEM((2, 3, 2 * BLK, HD), BF),
        pltpu.VMEM((8, TOPB * BLK), F32),
        pltpu.VMEM((NB, 2 * BLK, HD), BF),
        pltpu.VMEM((NB, 8, 128), F32),
        pltpu.VMEM((NB, 2 * BLK, HD), BF),
        pltpu.VMEM((NB, 2 * BLK, HD), BF),
        pltpu.VMEM((NB, 8, 128), F32),
        pltpu.VMEM((NB, 2 * BLK, HD), F32),
        pltpu.VMEM((NB, 2, 2 * BLK, 128), F32),
        dma((5,)),
        dma((3, 9)), dma((3, 9)),
        dma((NB, 9)), dma((NB, 9)),
        dma((2, 7, 3)), dma((2, 7, 3)),
        dma((2,)), dma((2,)),
        dma((NZ, 2)), dma((NZ, 2)),
        dma((3,)), dma((3,)),
        dma((4,)),
        dma((2,)), dma((2,)), dma((2,)), dma((2,)),
        dma((1,)), dma((1,)),
        dma((NB,)), dma((NB,)), dma((NB,)), dma((NB,)),
        dma((NB,)), dma((NB,)),
    ]
    return pl.pallas_call(
        kernel,
        out_shape=jax.ShapeDtypeStruct((ROWS, COLS), BF),
        in_specs=[hbm, hbm, hbm, hbm, hbm, vmem, smem, vmem, vmem],
        out_specs=vmem,
        scratch_shapes=scratch,
        compiler_params=pltpu.CompilerParams(
            collective_id=0, has_side_effects=True, vmem_limit_bytes=53 * 1024 * 1024 + 512 * 1024
        ),
        name="layer",
    )(tokens, query_weight, key_weight, value_weight, out_weight, req, idx, bias, far_bias)


def solution(mesh):
    placed = (P("kv", "tp"), P(None, "tp"), P(None, "tp"), P(None, "tp"), P(None, "tp"), P("kv", None))
    return jax.shard_map(local, mesh=mesh, in_specs=placed, out_specs=P("kv", "tp"), check_vma=False)
```

```python
import math

import jax
import jax.numpy as jnp
from jax import lax
from jax.experimental import pallas as pl
from jax.experimental.pallas import tpu as pltpu
from jax.sharding import PartitionSpec as P

HD = 128
BLK = 64
TOPB = 16
NB = 6
NX, NY, NZ = 4, 4, 16
ROWS = NB * BLK
COLS = 256
PER = 6
FAR = 4
OWN = NZ * PER
FLOOR = -1e30
MESH = pl.DeviceIdType.MESH
BF = jnp.bfloat16
F32 = jnp.float32
EXP_SCALE = HD ** (-0.5) * math.log2(math.e)


class Exchange:
    def __init__(self, buf, rows, x, c, kv, ssem, rsem):
        self.buf, self.rows, self.x, self.c, self.kv = buf, rows, x, c, kv
        self.ssem, self.rsem = ssem, rsem
        self.xp, self.xm, self.xo = (x + 1) % NX, (x + NX - 1) % NX, (x + 2) % NX
        self.pc = 1 - c
        self.sent = []

    def part(self, x, c, chunk, half=None):
        rows = self.rows if half is None else self.rows // 2
        start = chunk * self.rows + (0 if half is None else half * rows)
        return self.buf.at[x * 2 + c, pl.ds(start, rows), :]

    def copy(self, ref, chunk, kind, x, c):
        return pltpu.make_async_remote_copy(
            src_ref=ref, dst_ref=ref, send_sem=self.ssem.at[chunk, kind], recv_sem=self.rsem.at[chunk, kind],
            device_id={"kv": self.kv, "tp": x * 2 + c}, device_id_type=MESH,
        )

    def send(self, ref, chunk, kind, x, c):
        copy = self.copy(ref, chunk, kind, x, c)
        copy.start()
        self.sent.append(copy)

    def got(self, ref, chunk, kind):
        self.copy(ref, chunk, kind, self.x, self.pc).wait_recv()

    def own(self, k):
        ref = self.part(self.x, self.c, k)
        self.send(ref, k, 0, self.xp, self.c)
        self.send(ref, k, 1, self.xm, self.c)
        self.send(ref, k, 2, self.x, self.pc)

    def direct(self, k):
        self.got(self.part(self.xm, self.c, k), k, 0)
        self.send(self.part(self.xm, self.c, k, 0), k, 3, self.xp, self.c)
        self.send(self.part(self.xm, self.c, k), k, 5, self.x, self.pc)
        self.got(self.part(self.xp, self.c, k), k, 1)
        self.send(self.part(self.xp, self.c, k, 1), k, 4, self.xm, self.c)
        self.send(self.part(self.xp, self.c, k), k, 6, self.x, self.pc)

    def relayed(self, k):
        for half in (0, 1):
            ref = self.part(self.xo, self.c, k, half)
            self.got(ref, k, 3 + half)
            self.send(ref, k, 7 + half, self.x, self.pc)

    def finish(self, k):
        self.got(self.part(self.x, self.pc, k), k, 2)
        self.got(self.part(self.xm, self.pc, k), k, 5)
        self.got(self.part(self.xp, self.pc, k), k, 6)
        self.got(self.part(self.xo, self.pc, k, 0), k, 7)
        self.got(self.part(self.xo, self.pc, k, 1), k, 8)

    def drain(self):
        for copy in self.sent:
            copy.wait_send()


def kernel(tok, wq, wk, wv, wo, req_in, idx_ref, bias_ref, far_bias, out_ref, *scratch):
    (xbuf, hbuf, wqkv, wos, qs, own, mid, pool, stage, kvs, rbuf, req_sm) = scratch[:12]
    units_f, units_b = scratch[12:19], scratch[19:26]
    (fpool, fkvs, qin, qrel, fbias, ret, lse, far_out, back_lse, acc, mass) = scratch[26:37]
    (lsem, a_s, a_r, e_s, e_r, zs, zr, ms, mr, ys, yr, rs, rr, smem_sem, q1s, q1r, q2s, q2r, bs, br, b2s, b2r,
     ls, lr) = scratch[37:]

    kv = lax.axis_index("kv")
    tp = lax.axis_index("tp")
    z, y = kv // NY, kv % NY
    x, c = tp // 2, tp % 2
    yp, ym, yo = (y + 1) % NY, (y + NY - 1) % NY, (y + 2) % NY
    zp, zm = (z + 1) % NZ, (z + NZ - 1) % NZ

    loads = [
        pltpu.make_async_copy(tok, xbuf.at[tp], lsem.at[0]),
        pltpu.make_async_copy(wq, wqkv.at[:, 0:256], lsem.at[1]),
        pltpu.make_async_copy(wk, wqkv.at[:, 256:384], lsem.at[2]),
        pltpu.make_async_copy(wv, wqkv.at[:, 384:512], lsem.at[3]),
        pltpu.make_async_copy(wo, wos, lsem.at[4]),
    ]
    for load in loads:
        load.start()

    def dev(zz, yy, tt):
        return {"kv": zz * NY + yy, "tp": tt}

    near = [
        dev(z, y, x * 2 + 1 - c), dev(z, y, ((x + 1) % NX) * 2 + c), dev(z, y, ((x + 3) % NX) * 2 + c),
        dev(z, yp, tp), dev(z, ym, tp), dev(z, yo, tp), dev(zp, y, tp), dev(zm, y, tp),
    ]
    barrier = pltpu.get_barrier_semaphore()
    for other in near:
        pl.semaphore_signal(barrier, inc=1, device_id=other, device_id_type=MESH)
    pl.semaphore_wait(barrier, len(near))

    sent = []

    def rcopy(src, dst, ssem, rsem, to):
        return pltpu.make_async_remote_copy(
            src_ref=src, dst_ref=dst, send_sem=ssem, recv_sem=rsem, device_id=to, device_id_type=MESH
        )

    def send(*args, only=None):
        copy = rcopy(*args)
        if only is None:
            copy.start()
        else:
            pl.when(only)(copy.start)
        sent.append((only, copy))

    def wait(*args, only):
        pl.when(only)(rcopy(*args).wait_recv)

    tokens = Exchange(xbuf, 2 * BLK, x, c, kv, a_s, a_r)
    loads[0].wait()
    for k in range(3):
        tokens.own(k)
    send(req_in.at[yp], rbuf.at[2], rs.at[2], rr.at[2], dev(z, yp, tp))
    send(req_in.at[yo], rbuf.at[1], rs.at[1], rr.at[1], dev(z, yo, tp))
    send(req_in.at[ym], rbuf.at[0], rs.at[0], rr.at[0], dev(z, ym, tp))
    send(far_bias, fbias, bs.at[0], br.at[0], dev(z, yo, tp))
    for load in loads[1:]:
        load.wait()

    def project(k):
        rows = pl.ds(k * 2 * BLK, 2 * BLK)
        total = None
        for t in range(8):
            term = jnp.dot(xbuf[t, rows, :], wqkv[t * COLS:(t + 1) * COLS, :], preferred_element_type=F32)
            total = term if total is None else total + term
        rounded = total.astype(BF)
        for i in range(2):
            b = 2 * k + i
            here = rounded[i * BLK:(i + 1) * BLK]
            own[b] = here[:, 256:512]
            pool[OWN + b] = here[:, 256:512]
            qs[b, 0:BLK, :] = here[:, 0:128]
            qs[b, BLK:2 * BLK, :] = here[:, 128:256]

    def goes_up(k):
        return (z >= k - 1) & (z < NZ - 1)

    def comes_up(k):
        return z >= k

    def goes_down(k):
        return (z + k - 1) % NZ <= 7

    def comes_down(k):
        return (z + k) % NZ <= 7

    def piece(s):
        return pl.ds(2 * s, 2)

    def fwd(k, s):
        src = own if k == 1 else units_f[k - 2]
        return (src.at[piece(s)], units_f[k - 1].at[piece(s)], zs.at[0, k - 1, s], zr.at[0, k - 1, s], dev(zp, y, tp))

    def bwd(k, s):
        src = own if k == 1 else units_b[k - 2]
        return (src.at[piece(s)], units_b[k - 1].at[piece(s)], zs.at[1, k - 1, s], zr.at[1, k - 1, s], dev(zm, y, tp))

    def mid_fwd():
        return (units_f[6].at[pl.ds(0, 3)], mid.at[pl.ds(0, 3)], ms.at[0], mr.at[0], dev(zp, y, tp))

    def mid_bwd():
        return (units_b[6].at[pl.ds(3, 3)], mid.at[pl.ds(3, 3)], ms.at[1], mr.at[1], dev(zm, y, tp))

    def finish_chunk(k):
        tokens.finish(k)
        project(k)
        send(*fwd(1, k), only=goes_up(1))
        send(*bwd(1, k), only=goes_down(1))

    for k in range(3):
        tokens.direct(k)
    for k in range(3):
        tokens.relayed(k)
        finish_chunk(k)

    def ship(i):
        to = dev(z, yp, tp) if i == 0 else dev(z, ym, tp)
        return (qs.at[pl.ds(3 * i, 3)], qrel.at[i], q1s.at[i], q1r.at[i], to)

    def ship_on(i):
        to = dev(z, yp, tp) if i == 0 else dev(z, ym, tp)
        return (qrel.at[i], qin.at[pl.ds(3 * i, 3)], q2s.at[i], q2r.at[i], to)

    send(*ship(0))
    send(*ship(1))

    mine = pltpu.make_async_copy(req_in.at[y], req_sm.at[0], smem_sem.at[0])
    mine.start()
    asked = []
    for i in range(3):
        rcopy(rbuf.at[i], rbuf.at[i], rs.at[i], rr.at[i], dev(z, yp, tp)).wait_recv()
        asked.append(pltpu.make_async_copy(rbuf.at[i], req_sm.at[i + 1], smem_sem.at[i + 1]))
        asked[-1].start()
    mine.wait()
    for copy in asked:
        copy.wait()

    def up(d):
        return (stage.at[d, pl.ds(0, 2)], pool.at[pl.ds(d * PER + 2, 2)], ys.at[d, 0], yr.at[d, 0], dev(z, yp, tp))

    def down(d):
        return (stage.at[d, pl.ds(2, 2)], pool.at[pl.ds(d * PER + 4, 2)], ys.at[d, 1], yr.at[d, 1], dev(z, ym, tp))

    def pick(unit, d):
        hz = (z + NZ - d) % NZ

        def block(role, slot):
            return unit[req_sm[role, 0, hz * 2 + slot]]

        @pl.when(z >= d)
        def _():
            stage[d, 0] = block(1, 0)
            stage[d, 1] = block(1, 1)
            stage[d, 2] = block(3, 0)
            stage[d, 3] = block(3, 1)
            fpool[2 * d] = block(2, 0)
            fpool[2 * d + 1] = block(2, 1)
            pool[d * PER] = block(0, 0)
            pool[d * PER + 1] = block(0, 1)

        send(*up(d), only=z >= d)
        send(*down(d), only=z >= d)

    pick(own, 0)
    for k in range(1, 8):
        for s in range(3):
            wait(*fwd(k, s), only=comes_up(k))
            if k < 7:
                send(*fwd(k + 1, s), only=goes_up(k + 1))
            elif s == 1:
                send(*mid_fwd(), only=goes_up(8))
            wait(*bwd(k, s), only=comes_down(k))
            if k < 7:
                send(*bwd(k + 1, s), only=goes_down(k + 1))
            elif s == 2:
                send(*mid_bwd(), only=goes_down(8))
        pick(units_f[k - 1], k)
        pick(units_b[k - 1], NZ - k)
        if k == 2:
            for i in range(2):
                rcopy(*ship(i)).wait_recv()
                send(*ship_on(i))
    wait(*mid_fwd(), only=comes_up(8))
    wait(*mid_bwd(), only=comes_down(8))
    pick(mid, 8)
    heads = Exchange(hbuf, 2 * BLK, x, c, kv, e_s, e_r)
    row = lax.broadcasted_iota(jnp.int32, (2 * BLK, 128), 0) % BLK
    col = lax.broadcasted_iota(jnp.int32, (2 * BLK, 128), 1)
    late = (col < BLK) & (col > row)

    def back(b):
        return (ret.at[b], far_out.at[b], b2s.at[b], b2r.at[b], dev(z, yo, tp))

    def back_mass(b):
        return (lse.at[b], back_lse.at[b], ls.at[b], lr.at[b], dev(z, yo, tp))

    def attend_far(b):
        here = fkvs.at[b % 2]
        for j in range(FAR, TOPB):
            here[(j - FAR) * BLK:(j - FAR + 1) * BLK, :] = fpool[req_sm[2, 1, b * TOPB + j]]
        scores = lax.dot_general(
            qin[b], here[:, 0:HD], (((1,), (1,)), ((), ())), preferred_element_type=F32
        ) + fbias[b:b + 1, FAR * BLK:]
        peak = jnp.maximum(jnp.max(scores, axis=1, keepdims=True), FLOOR)
        weights = jnp.exp2((scores - peak) * EXP_SCALE)
        total = jnp.maximum(jnp.sum(weights, axis=1, keepdims=True), 1e-30)
        part = jnp.dot(weights.astype(BF), here[:, HD:2 * HD], preferred_element_type=F32) / total
        ret[b] = part.astype(BF)
        size = peak * EXP_SCALE + jnp.log(total) * math.log2(math.e)
        lse[b] = jnp.transpose(jnp.broadcast_to(size, (2 * BLK, 128)))[0:8]
        send(*back(b))
        send(*back_mass(b))

    def attend(b):
        here = kvs.at[b % 2]
        for j in range(TOPB):
            here[j * BLK:(j + 1) * BLK, :] = pool[idx_ref[b, j]]
        scores = lax.dot_general(
            qs[b], here[:, 0:HD], (((1,), (1,)), ((), ())), preferred_element_type=F32
        ) + bias_ref[b:b + 1, :]
        scores = jnp.concatenate([jnp.where(late, -jnp.inf, scores[:, 0:128]), scores[:, 128:]], axis=1)
        peak = jnp.max(scores, axis=1, keepdims=True)
        weights = jnp.exp2((scores - peak) * EXP_SCALE)
        acc[b] = jnp.dot(weights.astype(BF), here[:, HD:2 * HD], preferred_element_type=F32)
        mass[b, 0] = jnp.broadcast_to(peak * EXP_SCALE, (2 * BLK, 128))
        mass[b, 1] = jnp.broadcast_to(jnp.sum(weights, axis=1, keepdims=True), (2 * BLK, 128))

    def merge(b):
        rcopy(*back(b)).wait_recv()
        rcopy(*back_mass(b)).wait_recv()
        size = jnp.transpose(jnp.broadcast_to(back_lse[b, 0:1, :], (128, 2 * BLK)))
        peak = mass[b, 0]
        top = jnp.maximum(peak, size)
        mine, theirs = jnp.exp2(peak - top), jnp.exp2(size - top)
        mixed = (acc[b] * mine + far_out[b].astype(F32) * theirs) / (mass[b, 1] * mine + theirs)
        mixed = mixed.astype(BF)
        rows = pl.ds(b * BLK, BLK)
        hbuf[tp, rows, 0:HD] = mixed[0:BLK]
        hbuf[tp, rows, HD:2 * HD] = mixed[BLK:2 * BLK]

    def output(b):
        rows = pl.ds(b * 2 * BLK, 2 * BLK)
        total = None
        for t in range(8):
            term = jnp.dot(hbuf[t, rows, :], wos[t * COLS:(t + 1) * COLS, :], preferred_element_type=F32)
            total = term if total is None else total + term
        out_ref[rows, :] = total.astype(BF)

    for i in range(2):
        rcopy(*ship_on(i)).wait_recv()
    rcopy(far_bias, fbias, bs.at[0], br.at[0], dev(z, yo, tp)).wait_recv()
    for b in range(NB):
        attend_far(b)
    for d in range(NZ):
        wait(*up(d), only=z >= d)
        wait(*down(d), only=z >= d)
    for b in range(NB):
        attend(b)
    for b in range(NB):
        merge(b)
        if b % 2 == 1:
            heads.own(b // 2)
    for b in range(3):
        heads.direct(b)
    for b in range(4):
        if b < 3:
            heads.relayed(b)
        if b > 0:
            heads.finish(b - 1)
            output(b - 1)

    tokens.drain()
    heads.drain()
    for only, copy in sent:
        if only is None:
            copy.wait_send()
        else:
            pl.when(only)(copy.wait_send)


def tables(chosen):
    device = lax.axis_index("kv")
    z, y = device // NY, device % NY
    holder = chosen // NB
    inner = chosen - holder * NB
    far_holder = holder[:, 4:].reshape(-1)
    far_inner = inner[:, 4:].reshape(-1)
    asked = far_holder[None, :] == jnp.arange(NZ * NY)[:, None]
    low = jnp.min(jnp.where(asked, far_inner[None, :], NB - 1), axis=1)
    high = jnp.max(jnp.where(asked, far_inner[None, :], 0), axis=1)
    both = jnp.stack([low, high], axis=1).reshape(NZ, NY, 2).transpose(1, 0, 2).reshape(NY, 1, 2 * NZ)
    second = jnp.any(
        (far_holder[None, :] == far_holder[:, None]) & (far_inner[None, :] < far_inner[:, None]), axis=1
    ).astype(jnp.int32)
    second = jnp.pad(second.reshape(NB, TOPB - 4), ((0, 0), (4, 0)))
    step = (z - holder // NY) % NZ
    turn = (holder % NY - y) % NY
    far = turn == 2
    place = jnp.where(turn == 0, 0, jnp.where(turn == 1, 4, 2))
    idx = jnp.where(holder == device, OWN + inner, jnp.where(far, OWN, step * PER + place + second))
    far_idx = jnp.where(far, 2 * step + second, 0).reshape(1, 1, NB * TOPB)
    far_row = jnp.broadcast_to(jnp.pad(far_idx, ((0, 0), (0, 0), (0, 128 - NB * TOPB))), (NY, 1, 128))
    req_row = jnp.pad(both, ((0, 0), (0, 0), (0, 128 - 2 * NZ)))
    req = jnp.concatenate([req_row, far_row, jnp.zeros((NY, 6, 128), jnp.int32)], axis=1)
    order = jnp.arange(TOPB)
    repeats = jnp.any(
        (chosen[:, :, None] == chosen[:, None, :]) & (order[None, None, :] < order[None, :, None]), axis=2
    )
    near_bias = jnp.where(repeats | far, -jnp.inf, 0.0).astype(F32)
    far_bias = jnp.where(far & ~repeats, 0.0, -jnp.inf).astype(F32)

    def spread(rows):
        return jnp.broadcast_to(rows[:, :, None], (NB, TOPB, BLK)).reshape(NB, TOPB * BLK)

    far_bias = jnp.pad(spread(far_bias), ((0, 2), (0, 0)))
    return req.astype(jnp.int32), idx.astype(jnp.int32), spread(near_bias), far_bias


def local(tokens, query_weight, key_weight, value_weight, out_weight, chosen):
    req, idx, bias, far_bias = tables(chosen)
    dma = pltpu.SemaphoreType.DMA
    hbm = pl.BlockSpec(memory_space=pl.ANY)
    vmem = pl.BlockSpec(memory_space=pltpu.VMEM)
    smem = pl.BlockSpec(memory_space=pltpu.SMEM)
    unit = pltpu.VMEM((NB, BLK, COLS), BF)
    scratch = [
        pltpu.VMEM((8, ROWS, COLS), BF),
        pltpu.VMEM((8, ROWS, COLS), BF),
        pltpu.VMEM((2048, 512), BF),
        pltpu.VMEM((2048, COLS), BF),
        pltpu.VMEM((NB, 2 * BLK, HD), BF),
        unit,
        unit,
        pltpu.VMEM((OWN + NB, BLK, COLS), BF),
        pltpu.VMEM((NZ, 4, BLK, COLS), BF),
        pltpu.VMEM((2, TOPB * BLK, COLS), BF),
        pltpu.VMEM((3, 8, 128), jnp.int32),
        pltpu.SMEM((4, 8, 128), jnp.int32),
        *([unit] * 14),
        pltpu.VMEM((2 * NZ, BLK, COLS), BF),
        pltpu.VMEM((2, (TOPB - FAR) * BLK, COLS), BF),
        pltpu.VMEM((NB, 2 * BLK, HD), BF),
        pltpu.VMEM((2, 3, 2 * BLK, HD), BF),
        pltpu.VMEM((8, TOPB * BLK), F32),
        pltpu.VMEM((NB, 2 * BLK, HD), BF),
        pltpu.VMEM((NB, 8, 128), F32),
        pltpu.VMEM((NB, 2 * BLK, HD), BF),
        pltpu.VMEM((NB, 8, 128), F32),
        pltpu.VMEM((NB, 2 * BLK, HD), F32),
        pltpu.VMEM((NB, 2, 2 * BLK, 128), F32),
        dma((5,)),
        dma((3, 9)), dma((3, 9)),
        dma((3, 9)), dma((3, 9)),
        dma((2, 7, 3)), dma((2, 7, 3)),
        dma((2,)), dma((2,)),
        dma((NZ, 2)), dma((NZ, 2)),
        dma((3,)), dma((3,)),
        dma((4,)),
        dma((2,)), dma((2,)), dma((2,)), dma((2,)),
        dma((1,)), dma((1,)),
        dma((NB,)), dma((NB,)),
        dma((NB,)), dma((NB,)),
    ]
    return pl.pallas_call(
        kernel,
        out_shape=jax.ShapeDtypeStruct((ROWS, COLS), BF),
        in_specs=[hbm, hbm, hbm, hbm, hbm, vmem, smem, vmem, vmem],
        out_specs=vmem,
        scratch_shapes=scratch,
        compiler_params=pltpu.CompilerParams(
            collective_id=0, has_side_effects=True, vmem_limit_bytes=53 * 1024 * 1024 + 512 * 1024
        ),
        name="layer",
    )(tokens, query_weight, key_weight, value_weight, out_weight, req, idx, bias, far_bias)


def solution(mesh):
    placed = (P("kv", "tp"), P(None, "tp"), P(None, "tp"), P(None, "tp"), P(None, "tp"), P("kv", None))
    return jax.shard_map(local, mesh=mesh, in_specs=placed, out_specs=P("kv", "tp"), check_vma=False)
```

```python
import math

import jax
import jax.numpy as jnp
from jax import lax
from jax.experimental import pallas as pl
from jax.experimental.pallas import tpu as pltpu
from jax.sharding import PartitionSpec as P

HD = 128
BLK = 64
TOPB = 16
NB = 6
NX, NY, NZ = 4, 4, 16
ROWS = NB * BLK
COLS = 256
PER = 6
FAR = 4
OWN = NZ * PER
FLOOR = -1e30
MESH = pl.DeviceIdType.MESH
BF = jnp.bfloat16
F32 = jnp.float32
EXP_SCALE = HD ** (-0.5) * math.log2(math.e)


class Exchange:
    def __init__(self, buf, rows, x, c, kv, ssem, rsem):
        self.buf, self.rows, self.x, self.c, self.kv = buf, rows, x, c, kv
        self.ssem, self.rsem = ssem, rsem
        self.xp, self.xm, self.xo = (x + 1) % NX, (x + NX - 1) % NX, (x + 2) % NX
        self.pc = 1 - c
        self.sent = []

    def part(self, x, c, chunk, half=None):
        rows = self.rows if half is None else self.rows // 2
        start = chunk * self.rows + (0 if half is None else half * rows)
        return self.buf.at[x * 2 + c, pl.ds(start, rows), :]

    def copy(self, ref, chunk, kind, x, c):
        return pltpu.make_async_remote_copy(
            src_ref=ref, dst_ref=ref, send_sem=self.ssem.at[chunk, kind], recv_sem=self.rsem.at[chunk, kind],
            device_id={"kv": self.kv, "tp": x * 2 + c}, device_id_type=MESH,
        )

    def send(self, ref, chunk, kind, x, c):
        copy = self.copy(ref, chunk, kind, x, c)
        copy.start()
        self.sent.append(copy)

    def got(self, ref, chunk, kind):
        self.copy(ref, chunk, kind, self.x, self.pc).wait_recv()

    def own(self, k):
        ref = self.part(self.x, self.c, k)
        self.send(ref, k, 0, self.xp, self.c)
        self.send(ref, k, 1, self.xm, self.c)
        self.send(ref, k, 2, self.x, self.pc)

    def direct(self, k):
        self.got(self.part(self.xm, self.c, k), k, 0)
        self.send(self.part(self.xm, self.c, k, 0), k, 3, self.xp, self.c)
        self.send(self.part(self.xm, self.c, k), k, 5, self.x, self.pc)
        self.got(self.part(self.xp, self.c, k), k, 1)
        self.send(self.part(self.xp, self.c, k, 1), k, 4, self.xm, self.c)
        self.send(self.part(self.xp, self.c, k), k, 6, self.x, self.pc)

    def relayed(self, k):
        for half in (0, 1):
            ref = self.part(self.xo, self.c, k, half)
            self.got(ref, k, 3 + half)
            self.send(ref, k, 7 + half, self.x, self.pc)

    def finish(self, k):
        self.got(self.part(self.x, self.pc, k), k, 2)
        self.got(self.part(self.xm, self.pc, k), k, 5)
        self.got(self.part(self.xp, self.pc, k), k, 6)
        self.got(self.part(self.xo, self.pc, k, 0), k, 7)
        self.got(self.part(self.xo, self.pc, k, 1), k, 8)

    def drain(self):
        for copy in self.sent:
            copy.wait_send()


def split(name):
    holder = (name * 10923) >> 16
    return holder, name - NB * holder


def fill_bias(bias, half, b, names, elsewhere):
    value = []
    for j, name in enumerate(names):
        out = elsewhere(split(name)[0])
        for earlier in names[:j]:
            out = out | (earlier == name)
        value.append(jnp.where(out, -jnp.inf, 0.0).astype(F32))
    for i in range(len(names) // 2):
        bias[b:b + 1, i * 128:(i + 1) * 128] = jnp.where(half, value[2 * i], value[2 * i + 1])


def kernel(tok, wq, wk, wv, wo, chosen_in, out_ref, *scratch):
    (xbuf, hbuf, wqkv, wos, qs, own, mid, pool, stage, kvs, rbuf, req_sm) = scratch[:12]
    units_f, units_b = scratch[12:19], scratch[19:26]
    (fpool, fkvs, qin, qrel, fbias, ret, lse, far_out, back_lse, acc, mass, ask, bias, chosen) = scratch[26:40]
    (lsem, a_s, a_r, e_s, e_r, zs, zr, ms, mr, ys, yr, rs, rr, smem_sem, q1s, q1r, q2s, q2r, b2s, b2r,
     ls, lr) = scratch[40:]

    kv = lax.axis_index("kv")
    tp = lax.axis_index("tp")
    z, y = kv // NY, kv % NY
    x, c = tp // 2, tp % 2
    yp, ym, yo = (y + 1) % NY, (y + NY - 1) % NY, (y + 2) % NY
    zp, zm = (z + 1) % NZ, (z + NZ - 1) % NZ

    loads = [
        pltpu.make_async_copy(tok, xbuf.at[tp], lsem.at[0]),
        pltpu.make_async_copy(wq, wqkv.at[:, 0:256], lsem.at[1]),
        pltpu.make_async_copy(wk, wqkv.at[:, 256:384], lsem.at[2]),
        pltpu.make_async_copy(wv, wqkv.at[:, 384:512], lsem.at[3]),
        pltpu.make_async_copy(wo, wos, lsem.at[4]),
        pltpu.make_async_copy(chosen_in, chosen, lsem.at[5]),
    ]
    for load in (loads[5], *loads[:5]):
        load.start()

    def dev(zz, yy, tt):
        return {"kv": zz * NY + yy, "tp": tt}

    near = [
        dev(z, y, x * 2 + 1 - c), dev(z, y, ((x + 1) % NX) * 2 + c), dev(z, y, ((x + 3) % NX) * 2 + c),
        dev(z, yp, tp), dev(z, ym, tp), dev(z, yo, tp), dev(zp, y, tp), dev(zm, y, tp),
    ]
    barrier = pltpu.get_barrier_semaphore()
    for other in near:
        pl.semaphore_signal(barrier, inc=1, device_id=other, device_id_type=MESH)

    lane = lax.broadcasted_iota(jnp.int32, (8, 128), 1)
    sub = lax.broadcasted_iota(jnp.int32, (8, 128), 0)
    half = lax.broadcasted_iota(jnp.int32, (1, 128), 1) < BLK
    loads[5].wait()
    low = jnp.full((8, 128), NB - 1, jnp.int32)
    high = jnp.zeros((8, 128), jnp.int32)
    listed = jnp.zeros((8, 128), jnp.int32)
    for b in range(NB):
        names = [chosen[b, j] for j in range(TOPB)]
        for j in range(TOPB):
            holder, inner = split(names[j])
            listed = jnp.where(lane == b * TOPB + j, names[j], listed)
            if j >= FAR:
                low = jnp.where(lane == holder, jnp.minimum(low, inner), low)
                high = jnp.where(lane == holder, jnp.maximum(high, inner), high)
        fill_bias(bias, half, b, names, lambda holder: (holder & (NY - 1)) == yo)
    ask[...] = jnp.where(sub == 0, low, jnp.where(sub == 1, high, listed))
    pl.semaphore_wait(barrier, len(near))

    sent = []

    def rcopy(src, dst, ssem, rsem, to):
        return pltpu.make_async_remote_copy(
            src_ref=src, dst_ref=dst, send_sem=ssem, recv_sem=rsem, device_id=to, device_id_type=MESH
        )

    def send(*args, only=None):
        copy = rcopy(*args)
        if only is None:
            copy.start()
        else:
            pl.when(only)(copy.start)
        sent.append((only, copy))

    def wait(*args, only):
        pl.when(only)(rcopy(*args).wait_recv)

    tokens = Exchange(xbuf, 2 * BLK, x, c, kv, a_s, a_r)
    loads[0].wait()
    for k in range(3):
        tokens.own(k)
    send(ask, rbuf.at[2], rs.at[2], rr.at[2], dev(z, yp, tp))
    send(ask, rbuf.at[1], rs.at[1], rr.at[1], dev(z, yo, tp))
    send(ask, rbuf.at[0], rs.at[0], rr.at[0], dev(z, ym, tp))
    for load in loads[1:5]:
        load.wait()

    def project(k):
        rows = pl.ds(k * 2 * BLK, 2 * BLK)
        total = None
        for t in range(8):
            term = jnp.dot(xbuf[t, rows, :], wqkv[t * COLS:(t + 1) * COLS, :], preferred_element_type=F32)
            total = term if total is None else total + term
        rounded = total.astype(BF)
        for i in range(2):
            b = 2 * k + i
            here = rounded[i * BLK:(i + 1) * BLK]
            own[b] = here[:, 256:512]
            pool[OWN + b] = here[:, 256:512]
            qs[b, 0:BLK, :] = here[:, 0:128]
            qs[b, BLK:2 * BLK, :] = here[:, 128:256]

    def goes_up(k):
        return (z >= k - 1) & (z < NZ - 1)

    def comes_up(k):
        return z >= k

    def goes_down(k):
        return (z + k - 1) % NZ <= 7

    def comes_down(k):
        return (z + k) % NZ <= 7

    def piece(s):
        return pl.ds(2 * s, 2)

    def fwd(k, s):
        src = own if k == 1 else units_f[k - 2]
        return (src.at[piece(s)], units_f[k - 1].at[piece(s)], zs.at[0, k - 1, s], zr.at[0, k - 1, s], dev(zp, y, tp))

    def bwd(k, s):
        src = own if k == 1 else units_b[k - 2]
        return (src.at[piece(s)], units_b[k - 1].at[piece(s)], zs.at[1, k - 1, s], zr.at[1, k - 1, s], dev(zm, y, tp))

    def mid_fwd():
        return (units_f[6].at[pl.ds(0, 3)], mid.at[pl.ds(0, 3)], ms.at[0], mr.at[0], dev(zp, y, tp))

    def mid_bwd():
        return (units_b[6].at[pl.ds(3, 3)], mid.at[pl.ds(3, 3)], ms.at[1], mr.at[1], dev(zm, y, tp))

    def finish_chunk(k):
        tokens.finish(k)
        project(k)
        send(*fwd(1, k), only=goes_up(1))
        send(*bwd(1, k), only=goes_down(1))

    for k in range(3):
        tokens.direct(k)
    for k in range(3):
        tokens.relayed(k)
        finish_chunk(k)

    def ship(i):
        to = dev(z, yp, tp) if i == 0 else dev(z, ym, tp)
        return (qs.at[pl.ds(3 * i, 3)], qrel.at[i], q1s.at[i], q1r.at[i], to)

    def ship_on(i):
        to = dev(z, yp, tp) if i == 0 else dev(z, ym, tp)
        return (qrel.at[i], qin.at[pl.ds(3 * i, 3)], q2s.at[i], q2r.at[i], to)

    send(*ship(0))
    send(*ship(1))

    mine = pltpu.make_async_copy(ask, req_sm.at[0], smem_sem.at[0])
    mine.start()
    asked = []
    for i in range(3):
        rcopy(rbuf.at[i], rbuf.at[i], rs.at[i], rr.at[i], dev(z, yp, tp)).wait_recv()
        asked.append(pltpu.make_async_copy(rbuf.at[i], req_sm.at[i + 1], smem_sem.at[i + 1]))
        asked[-1].start()
    mine.wait()
    for copy in asked:
        copy.wait()

    def up(d):
        return (stage.at[d, pl.ds(0, 2)], pool.at[pl.ds(d * PER + 2, 2)], ys.at[d, 0], yr.at[d, 0], dev(z, yp, tp))

    def down(d):
        return (stage.at[d, pl.ds(2, 2)], pool.at[pl.ds(d * PER + 4, 2)], ys.at[d, 1], yr.at[d, 1], dev(z, ym, tp))

    def pick(unit, d):
        hz = (z + NZ - d) % NZ

        def block(role, slot):
            return unit[req_sm[role, slot, hz * NY + y]]

        @pl.when(z >= d)
        def _():
            stage[d, 0] = block(1, 0)
            stage[d, 1] = block(1, 1)
            stage[d, 2] = block(3, 0)
            stage[d, 3] = block(3, 1)
            fpool[2 * d] = block(2, 0)
            fpool[2 * d + 1] = block(2, 1)
            pool[d * PER] = block(0, 0)
            pool[d * PER + 1] = block(0, 1)

        send(*up(d), only=z >= d)
        send(*down(d), only=z >= d)

    pick(own, 0)
    for k in range(1, 8):
        for s in range(3):
            wait(*fwd(k, s), only=comes_up(k))
            if k < 7:
                send(*fwd(k + 1, s), only=goes_up(k + 1))
            elif s == 1:
                send(*mid_fwd(), only=goes_up(8))
            wait(*bwd(k, s), only=comes_down(k))
            if k < 7:
                send(*bwd(k + 1, s), only=goes_down(k + 1))
            elif s == 2:
                send(*mid_bwd(), only=goes_down(8))
        pick(units_f[k - 1], k)
        pick(units_b[k - 1], NZ - k)
        if k == 2:
            for i in range(2):
                rcopy(*ship(i)).wait_recv()
                send(*ship_on(i))
        if k == 3:
            for b in range(NB):
                names = [req_sm[2, 2, b * TOPB + j] for j in range(FAR, TOPB)]
                fill_bias(fbias, half, b, names, lambda holder: (holder & (NY - 1)) != y)
    wait(*mid_fwd(), only=comes_up(8))
    wait(*mid_bwd(), only=comes_down(8))
    pick(mid, 8)
    heads = Exchange(hbuf, 2 * BLK, x, c, kv, e_s, e_r)
    row = lax.broadcasted_iota(jnp.int32, (2 * BLK, 128), 0) % BLK
    col = lax.broadcasted_iota(jnp.int32, (2 * BLK, 128), 1)
    late = (col < BLK) & (col > row)

    def back(b):
        return (ret.at[b], far_out.at[b], b2s.at[b], b2r.at[b], dev(z, yo, tp))

    def back_mass(b):
        return (lse.at[b], back_lse.at[b], ls.at[b], lr.at[b], dev(z, yo, tp))

    def step_of(holder):
        return (z + NZ - (holder >> 2)) & (NZ - 1)

    def attend_far(b):
        here = fkvs.at[b % 2]
        for j in range(FAR, TOPB):
            holder, inner = split(req_sm[2, 2, b * TOPB + j])
            place = 2 * step_of(holder) + (inner != req_sm[2, 0, holder]).astype(jnp.int32)
            place = jnp.where((holder & (NY - 1)) == y, place, 0)
            here[(j - FAR) * BLK:(j - FAR + 1) * BLK, :] = fpool[place]
        scores = lax.dot_general(
            qin[b], here[:, 0:HD], (((1,), (1,)), ((), ())), preferred_element_type=F32
        ) + fbias[b:b + 1, :]
        peak = jnp.maximum(jnp.max(scores, axis=1, keepdims=True), FLOOR)
        weights = jnp.exp2((scores - peak) * EXP_SCALE)
        total = jnp.maximum(jnp.sum(weights, axis=1, keepdims=True), 1e-30)
        part = jnp.dot(weights.astype(BF), here[:, HD:2 * HD], preferred_element_type=F32) / total
        ret[b] = part.astype(BF)
        size = peak * EXP_SCALE + jnp.log(total) * math.log2(math.e)
        lse[b] = jnp.transpose(jnp.broadcast_to(size, (2 * BLK, 128)))[0:8]
        send(*back(b))
        send(*back_mass(b))

    def attend(b):
        here = kvs.at[b % 2]
        for j in range(TOPB):
            holder, inner = split(chosen[b, j])
            if j < FAR:
                place = OWN + inner
            else:
                turn = holder & (NY - 1)
                slot = jnp.where(turn == y, 0, jnp.where(turn == yp, 4, 2))
                slot = slot + (inner != req_sm[0, 0, holder]).astype(jnp.int32)
                place = jnp.where(turn == yo, OWN, step_of(holder) * PER + slot)
                place = jnp.where(holder == kv, OWN + inner, place)
            here[j * BLK:(j + 1) * BLK, :] = pool[place]
        scores = lax.dot_general(
            qs[b], here[:, 0:HD], (((1,), (1,)), ((), ())), preferred_element_type=F32
        ) + bias[b:b + 1, :]
        scores = jnp.concatenate([jnp.where(late, -jnp.inf, scores[:, 0:128]), scores[:, 128:]], axis=1)
        peak = jnp.max(scores, axis=1, keepdims=True)
        weights = jnp.exp2((scores - peak) * EXP_SCALE)
        acc[b] = jnp.dot(weights.astype(BF), here[:, HD:2 * HD], preferred_element_type=F32)
        mass[b, 0] = jnp.broadcast_to(peak * EXP_SCALE, (2 * BLK, 128))
        mass[b, 1] = jnp.broadcast_to(jnp.sum(weights, axis=1, keepdims=True), (2 * BLK, 128))

    def merge(b):
        rcopy(*back(b)).wait_recv()
        rcopy(*back_mass(b)).wait_recv()
        size = jnp.transpose(jnp.broadcast_to(back_lse[b, 0:1, :], (128, 2 * BLK)))
        peak = mass[b, 0]
        top = jnp.maximum(peak, size)
        mine, theirs = jnp.exp2(peak - top), jnp.exp2(size - top)
        mixed = (acc[b] * mine + far_out[b].astype(F32) * theirs) / (mass[b, 1] * mine + theirs)
        mixed = mixed.astype(BF)
        rows = pl.ds(b * BLK, BLK)
        hbuf[tp, rows, 0:HD] = mixed[0:BLK]
        hbuf[tp, rows, HD:2 * HD] = mixed[BLK:2 * BLK]

    def output(b):
        rows = pl.ds(b * 2 * BLK, 2 * BLK)
        total = None
        for t in range(8):
            term = jnp.dot(hbuf[t, rows, :], wos[t * COLS:(t + 1) * COLS, :], preferred_element_type=F32)
            total = term if total is None else total + term
        out_ref[rows, :] = total.astype(BF)

    for i in range(2):
        rcopy(*ship_on(i)).wait_recv()
    for b in range(NB):
        attend_far(b)
    for d in range(NZ):
        wait(*up(d), only=z >= d)
        wait(*down(d), only=z >= d)
    for b in range(NB):
        attend(b)
    for b in range(NB):
        merge(b)
        if b % 2 == 1:
            heads.own(b // 2)
    for b in range(3):
        heads.direct(b)
    for b in range(4):
        if b < 3:
            heads.relayed(b)
        if b > 0:
            heads.finish(b - 1)
            output(b - 1)

    tokens.drain()
    heads.drain()
    for only, copy in sent:
        if only is None:
            copy.wait_send()
        else:
            pl.when(only)(copy.wait_send)


def local(tokens, query_weight, key_weight, value_weight, out_weight, chosen):
    dma = pltpu.SemaphoreType.DMA
    hbm = pl.BlockSpec(memory_space=pl.ANY)
    vmem = pl.BlockSpec(memory_space=pltpu.VMEM)
    unit = pltpu.VMEM((NB, BLK, COLS), BF)
    scratch = [
        pltpu.VMEM((8, ROWS, COLS), BF),
        pltpu.VMEM((8, ROWS, COLS), BF),
        pltpu.VMEM((2048, 512), BF),
        pltpu.VMEM((2048, COLS), BF),
        pltpu.VMEM((NB, 2 * BLK, HD), BF),
        unit,
        unit,
        pltpu.VMEM((OWN + NB, BLK, COLS), BF),
        pltpu.VMEM((NZ, 4, BLK, COLS), BF),
        pltpu.VMEM((2, TOPB * BLK, COLS), BF),
        pltpu.VMEM((3, 8, 128), jnp.int32),
        pltpu.SMEM((4, 8, 128), jnp.int32),
        *([unit] * 14),
        pltpu.VMEM((2 * NZ, BLK, COLS), BF),
        pltpu.VMEM((2, (TOPB - FAR) * BLK, COLS), BF),
        pltpu.VMEM((NB, 2 * BLK, HD), BF),
        pltpu.VMEM((2, 3, 2 * BLK, HD), BF),
        pltpu.VMEM((8, (TOPB - FAR) * BLK), F32),
        pltpu.VMEM((NB, 2 * BLK, HD), BF),
        pltpu.VMEM((NB, 8, 128), F32),
        pltpu.VMEM((NB, 2 * BLK, HD), BF),
        pltpu.VMEM((NB, 8, 128), F32),
        pltpu.VMEM((NB, 2 * BLK, HD), F32),
        pltpu.VMEM((NB, 2, 2 * BLK, 128), F32),
        pltpu.VMEM((8, 128), jnp.int32),
        pltpu.VMEM((8, TOPB * BLK), F32),
        pltpu.SMEM((NB, TOPB), jnp.int32),
        dma((6,)),
        dma((3, 9)), dma((3, 9)),
        dma((3, 9)), dma((3, 9)),
        dma((2, 7, 3)), dma((2, 7, 3)),
        dma((2,)), dma((2,)),
        dma((NZ, 2)), dma((NZ, 2)),
        dma((3,)), dma((3,)),
        dma((4,)),
        dma((2,)), dma((2,)), dma((2,)), dma((2,)),
        dma((NB,)), dma((NB,)),
        dma((NB,)), dma((NB,)),
    ]
    return pl.pallas_call(
        kernel,
        out_shape=jax.ShapeDtypeStruct((ROWS, COLS), BF),
        in_specs=[hbm, hbm, hbm, hbm, hbm, hbm],
        out_specs=vmem,
        scratch_shapes=scratch,
        compiler_params=pltpu.CompilerParams(
            collective_id=0, has_side_effects=True, vmem_limit_bytes=53 * 1024 * 1024 + 672 * 1024
        ),
        name="layer",
    )(tokens, query_weight, key_weight, value_weight, out_weight, chosen)


def solution(mesh):
    placed = (P("kv", "tp"), P(None, "tp"), P(None, "tp"), P(None, "tp"), P(None, "tp"), P("kv", None))
    return jax.shard_map(local, mesh=mesh, in_specs=placed, out_specs=P("kv", "tp"), check_vma=False)
```

```python
import math

import jax
import jax.numpy as jnp
from jax import lax
from jax.experimental import pallas as pl
from jax.experimental.pallas import tpu as pltpu
from jax.sharding import PartitionSpec as P

HD = 128
BLK = 64
TOPB = 16
NB = 6
NX, NY, NZ = 4, 4, 16
ROWS = NB * BLK
COLS = 256
PER = 6
FAR = 4
OWN = NZ * PER
FLOOR = -1e30
MESH = pl.DeviceIdType.MESH
BF = jnp.bfloat16
F32 = jnp.float32
EXP_SCALE = HD ** (-0.5) * math.log2(math.e)


class Exchange:
    def __init__(self, buf, rows, x, c, kv, ssem, rsem):
        self.buf, self.rows, self.x, self.c, self.kv = buf, rows, x, c, kv
        self.ssem, self.rsem = ssem, rsem
        self.xp, self.xm, self.xo = (x + 1) % NX, (x + NX - 1) % NX, (x + 2) % NX
        self.pc = 1 - c
        self.sent = []

    def part(self, x, c, chunk, half=None):
        rows = self.rows if half is None else self.rows // 2
        start = chunk * self.rows + (0 if half is None else half * rows)
        return self.buf.at[x * 2 + c, pl.ds(start, rows), :]

    def copy(self, ref, chunk, kind, x, c):
        return pltpu.make_async_remote_copy(
            src_ref=ref, dst_ref=ref, send_sem=self.ssem.at[chunk, kind], recv_sem=self.rsem.at[chunk, kind],
            device_id={"kv": self.kv, "tp": x * 2 + c}, device_id_type=MESH,
        )

    def send(self, ref, chunk, kind, x, c):
        copy = self.copy(ref, chunk, kind, x, c)
        copy.start()
        self.sent.append(copy)

    def got(self, ref, chunk, kind):
        self.copy(ref, chunk, kind, self.x, self.pc).wait_recv()

    def own(self, k):
        ref = self.part(self.x, self.c, k)
        self.send(ref, k, 0, self.xp, self.c)
        self.send(ref, k, 1, self.xm, self.c)
        self.send(ref, k, 2, self.x, self.pc)

    def direct(self, k):
        self.got(self.part(self.xm, self.c, k), k, 0)
        self.send(self.part(self.xm, self.c, k, 0), k, 3, self.xp, self.c)
        self.send(self.part(self.xm, self.c, k), k, 5, self.x, self.pc)
        self.got(self.part(self.xp, self.c, k), k, 1)
        self.send(self.part(self.xp, self.c, k, 1), k, 4, self.xm, self.c)
        self.send(self.part(self.xp, self.c, k), k, 6, self.x, self.pc)

    def relayed(self, k):
        for half in (0, 1):
            ref = self.part(self.xo, self.c, k, half)
            self.got(ref, k, 3 + half)
        self.send(self.part(self.xo, self.c, k), k, 7, self.x, self.pc)

    def finish(self, k):
        self.got(self.part(self.x, self.pc, k), k, 2)
        self.got(self.part(self.xm, self.pc, k), k, 5)
        self.got(self.part(self.xp, self.pc, k), k, 6)
        self.got(self.part(self.xo, self.pc, k), k, 7)

    def drain(self):
        for copy in self.sent:
            copy.wait_send()


def split(name):
    holder = (name * 10923) >> 16
    return holder, name - NB * holder


def fill_bias(bias, half, b, names, elsewhere):
    value = []
    for j, name in enumerate(names):
        out = elsewhere(split(name)[0])
        for earlier in names[:j]:
            out = out | (earlier == name)
        value.append(jnp.where(out, -jnp.inf, 0.0).astype(F32))
    for i in range(len(names) // 2):
        bias[b:b + 1, i * 128:(i + 1) * 128] = jnp.where(half, value[2 * i], value[2 * i + 1])


def kernel(tok, wq, wk, wv, wo, chosen_in, out_ref, *scratch):
    (xbuf, hbuf, wqkv, wos, qs, own, mid, pool, stage, kvs, rbuf, req_sm) = scratch[:12]
    units_f, units_b = scratch[12:19], scratch[19:26]
    (fpool, fkvs, qin, qrel, fbias, ret, lse, far_out, back_lse, acc, mass, ask, bias, chosen) = scratch[26:40]
    (lsem, a_s, a_r, e_s, e_r, zs, zr, ms, mr, ys, yr, rs, rr, smem_sem, q1s, q1r, q2s, q2r, b2s, b2r,
     ls, lr) = scratch[40:]

    kv = lax.axis_index("kv")
    tp = lax.axis_index("tp")
    z, y = kv // NY, kv % NY
    x, c = tp // 2, tp % 2
    yp, ym, yo = (y + 1) % NY, (y + NY - 1) % NY, (y + 2) % NY
    zp, zm = (z + 1) % NZ, (z + NZ - 1) % NZ

    loads = [
        pltpu.make_async_copy(tok, xbuf.at[tp], lsem.at[0]),
        pltpu.make_async_copy(wq, wqkv.at[:, 0:256], lsem.at[1]),
        pltpu.make_async_copy(wk, wqkv.at[:, 256:384], lsem.at[2]),
        pltpu.make_async_copy(wv, wqkv.at[:, 384:512], lsem.at[3]),
        pltpu.make_async_copy(wo, wos, lsem.at[4]),
        pltpu.make_async_copy(chosen_in, chosen, lsem.at[5]),
    ]
    for load in (loads[5], *loads[:5]):
        load.start()

    def dev(zz, yy, tt):
        return {"kv": zz * NY + yy, "tp": tt}

    near = [
        dev(z, y, x * 2 + 1 - c), dev(z, y, ((x + 1) % NX) * 2 + c), dev(z, y, ((x + 3) % NX) * 2 + c),
        dev(z, yp, tp), dev(z, ym, tp), dev(z, yo, tp), dev(zp, y, tp), dev(zm, y, tp),
    ]
    barrier = pltpu.get_barrier_semaphore()
    for other in near:
        pl.semaphore_signal(barrier, inc=1, device_id=other, device_id_type=MESH)

    lane = lax.broadcasted_iota(jnp.int32, (8, 128), 1)
    sub = lax.broadcasted_iota(jnp.int32, (8, 128), 0)
    half = lax.broadcasted_iota(jnp.int32, (1, 128), 1) < BLK
    loads[5].wait()
    low = jnp.full((8, 128), NB - 1, jnp.int32)
    high = jnp.zeros((8, 128), jnp.int32)
    listed = jnp.zeros((8, 128), jnp.int32)
    for b in range(NB):
        names = [chosen[b, j] for j in range(TOPB)]
        for j in range(TOPB):
            holder, inner = split(names[j])
            listed = jnp.where(lane == b * TOPB + j, names[j], listed)
            if j >= FAR:
                low = jnp.where(lane == holder, jnp.minimum(low, inner), low)
                high = jnp.where(lane == holder, jnp.maximum(high, inner), high)
        fill_bias(bias, half, b, names, lambda holder: (holder & (NY - 1)) == yo)
    ask[...] = jnp.where(sub == 0, low, jnp.where(sub == 1, high, listed))
    pl.semaphore_wait(barrier, len(near))

    sent = []

    def rcopy(src, dst, ssem, rsem, to):
        return pltpu.make_async_remote_copy(
            src_ref=src, dst_ref=dst, send_sem=ssem, recv_sem=rsem, device_id=to, device_id_type=MESH
        )

    def send(*args, only=None):
        copy = rcopy(*args)
        if only is None:
            copy.start()
        else:
            pl.when(only)(copy.start)
        sent.append((only, copy))

    def wait(*args, only):
        pl.when(only)(rcopy(*args).wait_recv)

    tokens = Exchange(xbuf, 2 * BLK, x, c, kv, a_s, a_r)
    loads[0].wait()
    for k in range(3):
        tokens.own(k)
    send(ask, rbuf.at[2], rs.at[2], rr.at[2], dev(z, yp, tp))
    send(ask, rbuf.at[1], rs.at[1], rr.at[1], dev(z, yo, tp))
    send(ask, rbuf.at[0], rs.at[0], rr.at[0], dev(z, ym, tp))
    for load in loads[1:5]:
        load.wait()

    def project(k):
        rows = pl.ds(k * 2 * BLK, 2 * BLK)
        total = None
        for t in range(8):
            term = jnp.dot(xbuf[t, rows, :], wqkv[t * COLS:(t + 1) * COLS, :], preferred_element_type=F32)
            total = term if total is None else total + term
        rounded = total.astype(BF)
        for i in range(2):
            b = 2 * k + i
            here = rounded[i * BLK:(i + 1) * BLK]
            own[b] = here[:, 256:512]
            pool[OWN + b] = here[:, 256:512]
            qs[b, 0:BLK, :] = here[:, 0:128]
            qs[b, BLK:2 * BLK, :] = here[:, 128:256]

    def goes_up(k):
        return (z >= k - 1) & (z < NZ - 1)

    def comes_up(k):
        return z >= k

    def goes_down(k):
        return (z + k - 1) % NZ <= 7

    def comes_down(k):
        return (z + k) % NZ <= 7

    def piece(s):
        return pl.ds(2 * s, 2)

    def fwd(k, s):
        src = own if k == 1 else units_f[k - 2]
        return (src.at[piece(s)], units_f[k - 1].at[piece(s)], zs.at[0, k - 1, s], zr.at[0, k - 1, s], dev(zp, y, tp))

    def bwd(k, s):
        src = own if k == 1 else units_b[k - 2]
        return (src.at[piece(s)], units_b[k - 1].at[piece(s)], zs.at[1, k - 1, s], zr.at[1, k - 1, s], dev(zm, y, tp))

    def mid_fwd():
        return (units_f[6].at[pl.ds(0, 3)], mid.at[pl.ds(0, 3)], ms.at[0], mr.at[0], dev(zp, y, tp))

    def mid_bwd():
        return (units_b[6].at[pl.ds(3, 3)], mid.at[pl.ds(3, 3)], ms.at[1], mr.at[1], dev(zm, y, tp))

    def finish_chunk(k):
        tokens.finish(k)
        project(k)
        send(*fwd(1, k), only=goes_up(1))
        send(*bwd(1, k), only=goes_down(1))

    for k in range(3):
        tokens.direct(k)
    for k in range(3):
        tokens.relayed(k)
        finish_chunk(k)

    def ship(i):
        to = dev(z, yp, tp) if i == 0 else dev(z, ym, tp)
        return (qs.at[pl.ds(3 * i, 3)], qrel.at[i], q1s.at[i], q1r.at[i], to)

    def ship_on(i):
        to = dev(z, yp, tp) if i == 0 else dev(z, ym, tp)
        return (qrel.at[i], qin.at[pl.ds(3 * i, 3)], q2s.at[i], q2r.at[i], to)

    send(*ship(0))
    send(*ship(1))

    mine = pltpu.make_async_copy(ask, req_sm.at[0], smem_sem.at[0])
    mine.start()
    asked = []
    for i in range(3):
        rcopy(rbuf.at[i], rbuf.at[i], rs.at[i], rr.at[i], dev(z, yp, tp)).wait_recv()
        asked.append(pltpu.make_async_copy(rbuf.at[i], req_sm.at[i + 1], smem_sem.at[i + 1]))
        asked[-1].start()
    mine.wait()
    for copy in asked:
        copy.wait()

    def up(d):
        return (stage.at[d, pl.ds(0, 2)], pool.at[pl.ds(d * PER + 2, 2)], ys.at[d, 0], yr.at[d, 0], dev(z, yp, tp))

    def down(d):
        return (stage.at[d, pl.ds(2, 2)], pool.at[pl.ds(d * PER + 4, 2)], ys.at[d, 1], yr.at[d, 1], dev(z, ym, tp))

    def pick(unit, d):
        hz = (z + NZ - d) % NZ

        def block(role, slot):
            return unit[req_sm[role, slot, hz * NY + y]]

        @pl.when(z >= d)
        def _():
            stage[d, 0] = block(1, 0)
            stage[d, 1] = block(1, 1)
            stage[d, 2] = block(3, 0)
            stage[d, 3] = block(3, 1)
            fpool[2 * d] = block(2, 0)
            fpool[2 * d + 1] = block(2, 1)
            pool[d * PER] = block(0, 0)
            pool[d * PER + 1] = block(0, 1)

        send(*up(d), only=z >= d)
        send(*down(d), only=z >= d)

    pick(own, 0)
    for k in range(1, 8):
        for s in range(3):
            wait(*fwd(k, s), only=comes_up(k))
            if k < 7:
                send(*fwd(k + 1, s), only=goes_up(k + 1))
            elif s == 1:
                send(*mid_fwd(), only=goes_up(8))
            wait(*bwd(k, s), only=comes_down(k))
            if k < 7:
                send(*bwd(k + 1, s), only=goes_down(k + 1))
            elif s == 2:
                send(*mid_bwd(), only=goes_down(8))
        pick(units_f[k - 1], k)
        pick(units_b[k - 1], NZ - k)
        if k == 2:
            for i in range(2):
                rcopy(*ship(i)).wait_recv()
                send(*ship_on(i))
        if k == 3:
            for b in range(NB):
                names = [req_sm[2, 2, b * TOPB + j] for j in range(FAR, TOPB)]
                fill_bias(fbias, half, b, names, lambda holder: (holder & (NY - 1)) != y)
    wait(*mid_fwd(), only=comes_up(8))
    wait(*mid_bwd(), only=comes_down(8))
    pick(mid, 8)
    heads = Exchange(hbuf, 2 * BLK, x, c, kv, e_s, e_r)
    row = lax.broadcasted_iota(jnp.int32, (2 * BLK, 128), 0) % BLK
    col = lax.broadcasted_iota(jnp.int32, (2 * BLK, 128), 1)
    late = (col < BLK) & (col > row)

    def back(b):
        pair = pl.ds(2 * b, 2)
        return (ret.at[pair], far_out.at[pair], b2s.at[b], b2r.at[b], dev(z, yo, tp))

    def back_mass(b):
        pair = pl.ds(2 * b, 2)
        return (lse.at[pair], back_lse.at[pair], ls.at[b], lr.at[b], dev(z, yo, tp))

    def step_of(holder):
        return (z + NZ - (holder >> 2)) & (NZ - 1)

    def attend_far(b):
        here = fkvs.at[b % 2]
        for j in range(FAR, TOPB):
            holder, inner = split(req_sm[2, 2, b * TOPB + j])
            place = 2 * step_of(holder) + (inner != req_sm[2, 0, holder]).astype(jnp.int32)
            place = jnp.where((holder & (NY - 1)) == y, place, 0)
            here[(j - FAR) * BLK:(j - FAR + 1) * BLK, :] = fpool[place]
        scores = lax.dot_general(
            qin[b], here[:, 0:HD], (((1,), (1,)), ((), ())), preferred_element_type=F32
        ) + fbias[b:b + 1, :]
        peak = jnp.maximum(jnp.max(scores, axis=1, keepdims=True), FLOOR)
        weights = jnp.exp2((scores - peak) * EXP_SCALE)
        total = jnp.maximum(jnp.sum(weights, axis=1, keepdims=True), 1e-30)
        part = jnp.dot(weights.astype(BF), here[:, HD:2 * HD], preferred_element_type=F32) / total
        ret[b] = part.astype(BF)
        size = peak * EXP_SCALE + jnp.log(total) * math.log2(math.e)
        lse[b] = jnp.transpose(jnp.broadcast_to(size, (2 * BLK, 128)))[0:8]
        if b % 2 == 1:
            send(*back(b // 2))
            send(*back_mass(b // 2))

    def attend(b):
        here = kvs.at[b % 2]
        for j in range(TOPB):
            holder, inner = split(chosen[b, j])
            if j < FAR:
                place = OWN + inner
            else:
                turn = holder & (NY - 1)
                slot = jnp.where(turn == y, 0, jnp.where(turn == yp, 4, 2))
                slot = slot + (inner != req_sm[0, 0, holder]).astype(jnp.int32)
                place = jnp.where(turn == yo, OWN, step_of(holder) * PER + slot)
                place = jnp.where(holder == kv, OWN + inner, place)
            here[j * BLK:(j + 1) * BLK, :] = pool[place]
        scores = lax.dot_general(
            qs[b], here[:, 0:HD], (((1,), (1,)), ((), ())), preferred_element_type=F32
        ) + bias[b:b + 1, :]
        scores = jnp.concatenate([jnp.where(late, -jnp.inf, scores[:, 0:128]), scores[:, 128:]], axis=1)
        peak = jnp.max(scores, axis=1, keepdims=True)
        weights = jnp.exp2((scores - peak) * EXP_SCALE)
        acc[b] = jnp.dot(weights.astype(BF), here[:, HD:2 * HD], preferred_element_type=F32)
        mass[b, 0] = jnp.broadcast_to(peak * EXP_SCALE, (2 * BLK, 128))
        mass[b, 1] = jnp.broadcast_to(jnp.sum(weights, axis=1, keepdims=True), (2 * BLK, 128))

    def merge(b):
        if b % 2 == 0:
            rcopy(*back(b // 2)).wait_recv()
            rcopy(*back_mass(b // 2)).wait_recv()
        size = jnp.transpose(jnp.broadcast_to(back_lse[b, 0:1, :], (128, 2 * BLK)))
        peak = mass[b, 0]
        top = jnp.maximum(peak, size)
        mine, theirs = jnp.exp2(peak - top), jnp.exp2(size - top)
        mixed = (acc[b] * mine + far_out[b].astype(F32) * theirs) / (mass[b, 1] * mine + theirs)
        mixed = mixed.astype(BF)
        rows = pl.ds(b * BLK, BLK)
        hbuf[tp, rows, 0:HD] = mixed[0:BLK]
        hbuf[tp, rows, HD:2 * HD] = mixed[BLK:2 * BLK]

    def output(b):
        rows = pl.ds(b * 2 * BLK, 2 * BLK)
        total = None
        for t in range(8):
            term = jnp.dot(hbuf[t, rows, :], wos[t * COLS:(t + 1) * COLS, :], preferred_element_type=F32)
            total = term if total is None else total + term
        out_ref[rows, :] = total.astype(BF)

    for i in range(2):
        rcopy(*ship_on(i)).wait_recv()
    for b in range(NB):
        attend_far(b)
    for d in range(NZ):
        wait(*up(d), only=z >= d)
        wait(*down(d), only=z >= d)
    for b in range(NB):
        attend(b)
    for b in range(NB):
        merge(b)
        if b % 2 == 1:
            heads.own(b // 2)
    for b in range(3):
        heads.direct(b)
    for b in range(4):
        if b < 3:
            heads.relayed(b)
        if b > 0:
            heads.finish(b - 1)
            output(b - 1)

    tokens.drain()
    heads.drain()
    for only, copy in sent:
        if only is None:
            copy.wait_send()
        else:
            pl.when(only)(copy.wait_send)


def local(tokens, query_weight, key_weight, value_weight, out_weight, chosen):
    dma = pltpu.SemaphoreType.DMA
    hbm = pl.BlockSpec(memory_space=pl.ANY)
    vmem = pl.BlockSpec(memory_space=pltpu.VMEM)
    unit = pltpu.VMEM((NB, BLK, COLS), BF)
    scratch = [
        pltpu.VMEM((8, ROWS, COLS), BF),
        pltpu.VMEM((8, ROWS, COLS), BF),
        pltpu.VMEM((2048, 512), BF),
        pltpu.VMEM((2048, COLS), BF),
        pltpu.VMEM((NB, 2 * BLK, HD), BF),
        unit,
        unit,
        pltpu.VMEM((OWN + NB, BLK, COLS), BF),
        pltpu.VMEM((NZ, 4, BLK, COLS), BF),
        pltpu.VMEM((2, TOPB * BLK, COLS), BF),
        pltpu.VMEM((3, 8, 128), jnp.int32),
        pltpu.SMEM((4, 8, 128), jnp.int32),
        *([unit] * 14),
        pltpu.VMEM((2 * NZ, BLK, COLS), BF),
        pltpu.VMEM((2, (TOPB - FAR) * BLK, COLS), BF),
        pltpu.VMEM((NB, 2 * BLK, HD), BF),
        pltpu.VMEM((2, 3, 2 * BLK, HD), BF),
        pltpu.VMEM((8, (TOPB - FAR) * BLK), F32),
        pltpu.VMEM((NB, 2 * BLK, HD), BF),
        pltpu.VMEM((NB, 8, 128), F32),
        pltpu.VMEM((NB, 2 * BLK, HD), BF),
        pltpu.VMEM((NB, 8, 128), F32),
        pltpu.VMEM((NB, 2 * BLK, HD), F32),
        pltpu.VMEM((NB, 2, 2 * BLK, 128), F32),
        pltpu.VMEM((8, 128), jnp.int32),
        pltpu.VMEM((8, TOPB * BLK), F32),
        pltpu.SMEM((NB, TOPB), jnp.int32),
        dma((6,)),
        dma((3, 8)), dma((3, 8)),
        dma((3, 8)), dma((3, 8)),
        dma((2, 7, 3)), dma((2, 7, 3)),
        dma((2,)), dma((2,)),
        dma((NZ, 2)), dma((NZ, 2)),
        dma((3,)), dma((3,)),
        dma((4,)),
        dma((2,)), dma((2,)), dma((2,)), dma((2,)),
        dma((3,)), dma((3,)),
        dma((3,)), dma((3,)),
    ]
    return pl.pallas_call(
        kernel,
        out_shape=jax.ShapeDtypeStruct((ROWS, COLS), BF),
        in_specs=[hbm, hbm, hbm, hbm, hbm, hbm],
        out_specs=vmem,
        scratch_shapes=scratch,
        compiler_params=pltpu.CompilerParams(
            collective_id=0, has_side_effects=True, vmem_limit_bytes=53 * 1024 * 1024 + 672 * 1024
        ),
        name="layer",
    )(tokens, query_weight, key_weight, value_weight, out_weight, chosen)


def solution(mesh):
    placed = (P("kv", "tp"), P(None, "tp"), P(None, "tp"), P(None, "tp"), P(None, "tp"), P("kv", None))
    return jax.shard_map(local, mesh=mesh, in_specs=placed, out_specs=P("kv", "tp"), check_vma=False)
```

```python
import math

import jax
import jax.numpy as jnp
from jax import lax
from jax.experimental import pallas as pl
from jax.experimental.pallas import tpu as pltpu
from jax.sharding import PartitionSpec as P

HD = 128
BLK = 64
TOPB = 16
NB = 6
NX, NY, NZ = 4, 4, 16
ROWS = NB * BLK
COLS = 256
PER = 6
FAR = 4
OWN = NZ * PER
FLOOR = -1e30
MESH = pl.DeviceIdType.MESH
BF = jnp.bfloat16
F32 = jnp.float32
EXP_SCALE = HD ** (-0.5) * math.log2(math.e)


class Exchange:
    def __init__(self, buf, rows, x, c, kv, ssem, rsem):
        self.buf, self.rows, self.x, self.c, self.kv = buf, rows, x, c, kv
        self.ssem, self.rsem = ssem, rsem
        self.xp, self.xm, self.xo = (x + 1) % NX, (x + NX - 1) % NX, (x + 2) % NX
        self.pc = 1 - c
        self.sent = []

    def part(self, x, c, chunk, half=None):
        rows = self.rows if half is None else self.rows // 2
        start = chunk * self.rows + (0 if half is None else half * rows)
        return self.buf.at[x * 2 + c, pl.ds(start, rows), :]

    def copy(self, ref, chunk, kind, x, c):
        return pltpu.make_async_remote_copy(
            src_ref=ref, dst_ref=ref, send_sem=self.ssem.at[chunk, kind], recv_sem=self.rsem.at[chunk, kind],
            device_id={"kv": self.kv, "tp": x * 2 + c}, device_id_type=MESH,
        )

    def send(self, ref, chunk, kind, x, c):
        copy = self.copy(ref, chunk, kind, x, c)
        copy.start()
        self.sent.append(copy)

    def got(self, ref, chunk, kind):
        self.copy(ref, chunk, kind, self.x, self.pc).wait_recv()

    def own(self, k):
        ref = self.part(self.x, self.c, k)
        self.send(ref, k, 0, self.xp, self.c)
        self.send(ref, k, 1, self.xm, self.c)
        self.send(ref, k, 2, self.x, self.pc)

    def direct(self, k):
        self.got(self.part(self.xm, self.c, k), k, 0)
        self.send(self.part(self.xm, self.c, k, 0), k, 3, self.xp, self.c)
        self.send(self.part(self.xm, self.c, k), k, 5, self.x, self.pc)
        self.got(self.part(self.xp, self.c, k), k, 1)
        self.send(self.part(self.xp, self.c, k, 1), k, 4, self.xm, self.c)
        self.send(self.part(self.xp, self.c, k), k, 6, self.x, self.pc)

    def relayed(self, k):
        for half in (0, 1):
            ref = self.part(self.xo, self.c, k, half)
            self.got(ref, k, 3 + half)
        self.send(self.part(self.xo, self.c, k), k, 7, self.x, self.pc)

    def finish(self, k):
        self.got(self.part(self.x, self.pc, k), k, 2)
        self.got(self.part(self.xm, self.pc, k), k, 5)
        self.got(self.part(self.xp, self.pc, k), k, 6)
        self.got(self.part(self.xo, self.pc, k), k, 7)

    def drain(self):
        for copy in self.sent:
            copy.wait_send()


def split(name):
    holder = (name * 10923) >> 16
    return holder, name - NB * holder


def fill_bias(bias, half, b, names, elsewhere):
    value = []
    for j, name in enumerate(names):
        out = elsewhere(split(name)[0])
        for earlier in names[:j]:
            out = out | (earlier == name)
        value.append(jnp.where(out, -jnp.inf, 0.0).astype(F32))
    for i in range(len(names) // 2):
        bias[b:b + 1, i * 128:(i + 1) * 128] = jnp.where(half, value[2 * i], value[2 * i + 1])


def kernel(tok, wq, wk, wv, wo, chosen_in, out_ref, *scratch):
    (xbuf, hbuf, wqkv, wos, qs, own, mid, pool, stage, kvs, rbuf, req_sm) = scratch[:12]
    units_f, units_b = scratch[12:19], scratch[19:26]
    (fpool, fkvs, qin, qrel, fbias, ret, lse, far_out, back_lse, acc, mass, ask, bias, chosen) = scratch[26:40]
    (lsem, a_s, a_r, e_s, e_r, zs, zr, ms, mr, ys, yr, rs, rr, smem_sem, q1s, q1r, q2s, q2r, b2s, b2r,
     ls, lr) = scratch[40:]

    kv = lax.axis_index("kv")
    tp = lax.axis_index("tp")
    z, y = kv // NY, kv % NY
    x, c = tp // 2, tp % 2
    yp, ym, yo = (y + 1) % NY, (y + NY - 1) % NY, (y + 2) % NY
    zp, zm = (z + 1) % NZ, (z + NZ - 1) % NZ

    loads = [
        pltpu.make_async_copy(tok, xbuf.at[tp], lsem.at[0]),
        pltpu.make_async_copy(wq, wqkv.at[:, 0:256], lsem.at[1]),
        pltpu.make_async_copy(wk, wqkv.at[:, 256:384], lsem.at[2]),
        pltpu.make_async_copy(wv, wqkv.at[:, 384:512], lsem.at[3]),
        pltpu.make_async_copy(wo, wos, lsem.at[4]),
        pltpu.make_async_copy(chosen_in, chosen, lsem.at[5]),
    ]
    for load in (loads[5], *loads[:5]):
        load.start()

    def dev(zz, yy, tt):
        return {"kv": zz * NY + yy, "tp": tt}

    near = [
        dev(z, y, x * 2 + 1 - c), dev(z, y, ((x + 1) % NX) * 2 + c), dev(z, y, ((x + 3) % NX) * 2 + c),
        dev(z, yp, tp), dev(z, ym, tp), dev(z, yo, tp), dev(zp, y, tp), dev(zm, y, tp),
    ]
    barrier = pltpu.get_barrier_semaphore()
    for other in near:
        pl.semaphore_signal(barrier, inc=1, device_id=other, device_id_type=MESH)

    lane = lax.broadcasted_iota(jnp.int32, (8, 128), 1)
    sub = lax.broadcasted_iota(jnp.int32, (8, 128), 0)
    half = lax.broadcasted_iota(jnp.int32, (1, 128), 1) < BLK
    loads[5].wait()
    low = jnp.full((8, 128), NB - 1, jnp.int32)
    high = jnp.zeros((8, 128), jnp.int32)
    listed = jnp.zeros((8, 128), jnp.int32)
    for b in range(NB):
        names = [chosen[b, j] for j in range(TOPB)]
        for j in range(TOPB):
            holder, inner = split(names[j])
            listed = jnp.where(lane == b * TOPB + j, names[j], listed)
            if j >= FAR:
                low = jnp.where(lane == holder, jnp.minimum(low, inner), low)
                high = jnp.where(lane == holder, jnp.maximum(high, inner), high)
        fill_bias(bias, half, b, names, lambda holder: (holder & (NY - 1)) == yo)
    ask[...] = jnp.where(sub == 0, low, jnp.where(sub == 1, high, listed))
    pl.semaphore_wait(barrier, len(near))

    sent = []

    def rcopy(src, dst, ssem, rsem, to):
        return pltpu.make_async_remote_copy(
            src_ref=src, dst_ref=dst, send_sem=ssem, recv_sem=rsem, device_id=to, device_id_type=MESH
        )

    def send(*args, only=None):
        copy = rcopy(*args)
        if only is None:
            copy.start()
        else:
            pl.when(only)(copy.start)
        sent.append((only, copy))

    def wait(*args, only):
        pl.when(only)(rcopy(*args).wait_recv)

    tokens = Exchange(xbuf, 2 * BLK, x, c, kv, a_s, a_r)
    loads[0].wait()
    for k in range(3):
        tokens.own(k)
    send(ask, rbuf.at[2], rs.at[2], rr.at[2], dev(z, yp, tp))
    send(ask, rbuf.at[1], rs.at[1], rr.at[1], dev(z, yo, tp))
    send(ask, rbuf.at[0], rs.at[0], rr.at[0], dev(z, ym, tp))
    for load in loads[1:5]:
        load.wait()

    def project(k):
        rows = pl.ds(k * 2 * BLK, 2 * BLK)
        total = None
        for t in range(8):
            term = jnp.dot(xbuf[t, rows, :], wqkv[t * COLS:(t + 1) * COLS, :], preferred_element_type=F32)
            total = term if total is None else total + term
        rounded = total.astype(BF)
        for i in range(2):
            b = 2 * k + i
            here = rounded[i * BLK:(i + 1) * BLK]
            own[b] = here[:, 256:512]
            pool[OWN + b] = here[:, 256:512]
            qs[b, 0:BLK, :] = here[:, 0:128]
            qs[b, BLK:2 * BLK, :] = here[:, 128:256]

    def goes_up(k):
        return (z >= k - 1) & (z < NZ - 1)

    def comes_up(k):
        return z >= k

    def goes_down(k, s):
        return (z + k - 1) % NZ <= (6 if s == 0 else 7)

    def comes_down(k, s):
        return (z + k) % NZ <= (6 if s == 0 else 7)

    def piece(s):
        return pl.ds(2 * s, 2)

    def fwd(k, s):
        src = own if k == 1 else units_f[k - 2]
        return (src.at[piece(s)], units_f[k - 1].at[piece(s)], zs.at[0, k - 1, s], zr.at[0, k - 1, s], dev(zp, y, tp))

    def bwd(k, s):
        src = own if k == 1 else units_b[k - 2]
        return (src.at[piece(s)], units_b[k - 1].at[piece(s)], zs.at[1, k - 1, s], zr.at[1, k - 1, s], dev(zm, y, tp))

    def mid_fwd():
        return (units_f[6].at[pl.ds(0, 3)], mid.at[pl.ds(0, 3)], ms.at[0], mr.at[0], dev(zp, y, tp))

    def mid_bwd():
        return (units_b[6].at[pl.ds(3, 3)], mid.at[pl.ds(3, 3)], ms.at[1], mr.at[1], dev(zm, y, tp))

    def finish_chunk(k):
        tokens.finish(k)
        project(k)
        send(*fwd(1, k), only=goes_up(1))
        send(*bwd(1, k), only=goes_down(1, k))

    for k in range(3):
        tokens.direct(k)
    for k in range(3):
        tokens.relayed(k)
        finish_chunk(k)

    def ship(i):
        to = dev(z, yp, tp) if i == 0 else dev(z, ym, tp)
        return (qs.at[pl.ds(3 * i, 3)], qrel.at[i], q1s.at[i], q1r.at[i], to)

    def ship_on(i):
        to = dev(z, yp, tp) if i == 0 else dev(z, ym, tp)
        return (qrel.at[i], qin.at[pl.ds(3 * i, 3)], q2s.at[i], q2r.at[i], to)

    send(*ship(0))
    send(*ship(1))

    mine = pltpu.make_async_copy(ask, req_sm.at[0], smem_sem.at[0])
    mine.start()
    asked = []
    for i in range(3):
        rcopy(rbuf.at[i], rbuf.at[i], rs.at[i], rr.at[i], dev(z, yp, tp)).wait_recv()
        asked.append(pltpu.make_async_copy(rbuf.at[i], req_sm.at[i + 1], smem_sem.at[i + 1]))
        asked[-1].start()
    mine.wait()
    for copy in asked:
        copy.wait()

    def up(d):
        return (stage.at[d, pl.ds(0, 2)], pool.at[pl.ds(d * PER + 2, 2)], ys.at[d, 0], yr.at[d, 0], dev(z, yp, tp))

    def down(d):
        return (stage.at[d, pl.ds(2, 2)], pool.at[pl.ds(d * PER + 4, 2)], ys.at[d, 1], yr.at[d, 1], dev(z, ym, tp))

    def pick(unit, d):
        hz = (z + NZ - d) % NZ

        def block(role, slot):
            return unit[req_sm[role, slot, hz * NY + y]]

        @pl.when(z >= d)
        def _():
            stage[d, 0] = block(1, 0)
            stage[d, 1] = block(1, 1)
            stage[d, 2] = block(3, 0)
            stage[d, 3] = block(3, 1)
            fpool[2 * d] = block(2, 0)
            fpool[2 * d + 1] = block(2, 1)
            pool[d * PER] = block(0, 0)
            pool[d * PER + 1] = block(0, 1)

        send(*up(d), only=z >= d)
        send(*down(d), only=z >= d)

    pick(own, 0)
    for k in range(1, 8):
        for s in range(3):
            wait(*fwd(k, s), only=comes_up(k))
            if k < 7:
                send(*fwd(k + 1, s), only=goes_up(k + 1))
            elif s == 1:
                send(*mid_fwd(), only=goes_up(8))
            wait(*bwd(k, s), only=comes_down(k, s))
            if k < 7:
                send(*bwd(k + 1, s), only=goes_down(k + 1, s))
            elif s == 2:
                send(*mid_bwd(), only=goes_down(8, 2))
        pick(units_f[k - 1], k)
        pick(units_b[k - 1], NZ - k)
        if k == 2:
            for i in range(2):
                rcopy(*ship(i)).wait_recv()
                send(*ship_on(i))
        if k == 3:
            for b in range(NB):
                names = [req_sm[2, 2, b * TOPB + j] for j in range(FAR, TOPB)]
                fill_bias(fbias, half, b, names, lambda holder: (holder & (NY - 1)) != y)
    wait(*mid_fwd(), only=comes_up(8))
    wait(*mid_bwd(), only=comes_down(8, 2))
    pick(mid, 8)
    heads = Exchange(hbuf, 2 * BLK, x, c, kv, e_s, e_r)
    row = lax.broadcasted_iota(jnp.int32, (2 * BLK, 128), 0) % BLK
    col = lax.broadcasted_iota(jnp.int32, (2 * BLK, 128), 1)
    late = (col < BLK) & (col > row)

    def back(b):
        pair = pl.ds(2 * b, 2)
        return (ret.at[pair], far_out.at[pair], b2s.at[b], b2r.at[b], dev(z, yo, tp))

    def back_mass(b):
        pair = pl.ds(2 * b, 2)
        return (lse.at[pair], back_lse.at[pair], ls.at[b], lr.at[b], dev(z, yo, tp))

    def step_of(holder):
        return (z + NZ - (holder >> 2)) & (NZ - 1)

    def attend_far(b):
        here = fkvs.at[b % 2]
        for j in range(FAR, TOPB):
            holder, inner = split(req_sm[2, 2, b * TOPB + j])
            place = 2 * step_of(holder) + (inner != req_sm[2, 0, holder]).astype(jnp.int32)
            place = jnp.where((holder & (NY - 1)) == y, place, 0)
            here[(j - FAR) * BLK:(j - FAR + 1) * BLK, :] = fpool[place]
        scores = lax.dot_general(
            qin[b], here[:, 0:HD], (((1,), (1,)), ((), ())), preferred_element_type=F32
        ) + fbias[b:b + 1, :]
        peak = jnp.maximum(jnp.max(scores, axis=1, keepdims=True), FLOOR)
        weights = jnp.exp2((scores - peak) * EXP_SCALE)
        total = jnp.maximum(jnp.sum(weights, axis=1, keepdims=True), 1e-30)
        part = jnp.dot(weights.astype(BF), here[:, HD:2 * HD], preferred_element_type=F32) / total
        ret[b] = part.astype(BF)
        size = peak * EXP_SCALE + jnp.log(total) * math.log2(math.e)
        lse[b] = jnp.transpose(jnp.broadcast_to(size, (2 * BLK, 128)))[0:8]
        if b % 2 == 1:
            send(*back(b // 2))
            send(*back_mass(b // 2))

    def attend(b):
        here = kvs.at[b % 2]
        for j in range(TOPB):
            holder, inner = split(chosen[b, j])
            if j < FAR:
                place = OWN + inner
            else:
                turn = holder & (NY - 1)
                slot = jnp.where(turn == y, 0, jnp.where(turn == yp, 4, 2))
                slot = slot + (inner != req_sm[0, 0, holder]).astype(jnp.int32)
                place = jnp.where(turn == yo, OWN, step_of(holder) * PER + slot)
                place = jnp.where(holder == kv, OWN + inner, place)
            here[j * BLK:(j + 1) * BLK, :] = pool[place]
        scores = lax.dot_general(
            qs[b], here[:, 0:HD], (((1,), (1,)), ((), ())), preferred_element_type=F32
        ) + bias[b:b + 1, :]
        scores = jnp.concatenate([jnp.where(late, -jnp.inf, scores[:, 0:128]), scores[:, 128:]], axis=1)
        peak = jnp.max(scores, axis=1, keepdims=True)
        weights = jnp.exp2((scores - peak) * EXP_SCALE)
        acc[b] = jnp.dot(weights.astype(BF), here[:, HD:2 * HD], preferred_element_type=F32)
        mass[b, 0] = jnp.broadcast_to(peak * EXP_SCALE, (2 * BLK, 128))
        mass[b, 1] = jnp.broadcast_to(jnp.sum(weights, axis=1, keepdims=True), (2 * BLK, 128))

    def merge(b):
        if b % 2 == 0:
            rcopy(*back(b // 2)).wait_recv()
            rcopy(*back_mass(b // 2)).wait_recv()
        size = jnp.transpose(jnp.broadcast_to(back_lse[b, 0:1, :], (128, 2 * BLK)))
        peak = mass[b, 0]
        top = jnp.maximum(peak, size)
        mine, theirs = jnp.exp2(peak - top), jnp.exp2(size - top)
        mixed = (acc[b] * mine + far_out[b].astype(F32) * theirs) / (mass[b, 1] * mine + theirs)
        mixed = mixed.astype(BF)
        rows = pl.ds(b * BLK, BLK)
        hbuf[tp, rows, 0:HD] = mixed[0:BLK]
        hbuf[tp, rows, HD:2 * HD] = mixed[BLK:2 * BLK]

    def output(b):
        rows = pl.ds(b * 2 * BLK, 2 * BLK)
        total = None
        for t in range(8):
            term = jnp.dot(hbuf[t, rows, :], wos[t * COLS:(t + 1) * COLS, :], preferred_element_type=F32)
            total = term if total is None else total + term
        out_ref[rows, :] = total.astype(BF)

    for i in range(2):
        rcopy(*ship_on(i)).wait_recv()
    for b in range(NB):
        attend_far(b)
    for d in range(NZ):
        wait(*up(d), only=z >= d)
        wait(*down(d), only=z >= d)
    for b in range(NB):
        attend(b)
    for b in range(NB):
        merge(b)
        if b % 2 == 1:
            heads.own(b // 2)
    for b in range(3):
        heads.direct(b)
    for b in range(4):
        if b < 3:
            heads.relayed(b)
        if b > 0:
            heads.finish(b - 1)
            output(b - 1)

    tokens.drain()
    heads.drain()
    for only, copy in sent:
        if only is None:
            copy.wait_send()
        else:
            pl.when(only)(copy.wait_send)


def local(tokens, query_weight, key_weight, value_weight, out_weight, chosen):
    dma = pltpu.SemaphoreType.DMA
    hbm = pl.BlockSpec(memory_space=pl.ANY)
    vmem = pl.BlockSpec(memory_space=pltpu.VMEM)
    unit = pltpu.VMEM((NB, BLK, COLS), BF)
    scratch = [
        pltpu.VMEM((8, ROWS, COLS), BF),
        pltpu.VMEM((8, ROWS, COLS), BF),
        pltpu.VMEM((2048, 512), BF),
        pltpu.VMEM((2048, COLS), BF),
        pltpu.VMEM((NB, 2 * BLK, HD), BF),
        unit,
        unit,
        pltpu.VMEM((OWN + NB, BLK, COLS), BF),
        pltpu.VMEM((NZ, 4, BLK, COLS), BF),
        pltpu.VMEM((2, TOPB * BLK, COLS), BF),
        pltpu.VMEM((3, 8, 128), jnp.int32),
        pltpu.SMEM((4, 8, 128), jnp.int32),
        *([unit] * 14),
        pltpu.VMEM((2 * NZ, BLK, COLS), BF),
        pltpu.VMEM((2, (TOPB - FAR) * BLK, COLS), BF),
        pltpu.VMEM((NB, 2 * BLK, HD), BF),
        pltpu.VMEM((2, 3, 2 * BLK, HD), BF),
        pltpu.VMEM((8, (TOPB - FAR) * BLK), F32),
        pltpu.VMEM((NB, 2 * BLK, HD), BF),
        pltpu.VMEM((NB, 8, 128), F32),
        pltpu.VMEM((NB, 2 * BLK, HD), BF),
        pltpu.VMEM((NB, 8, 128), F32),
        pltpu.VMEM((NB, 2 * BLK, HD), F32),
        pltpu.VMEM((NB, 2, 2 * BLK, 128), F32),
        pltpu.VMEM((8, 128), jnp.int32),
        pltpu.VMEM((8, TOPB * BLK), F32),
        pltpu.SMEM((NB, TOPB), jnp.int32),
        dma((6,)),
        dma((3, 8)), dma((3, 8)),
        dma((3, 8)), dma((3, 8)),
        dma((2, 7, 3)), dma((2, 7, 3)),
        dma((2,)), dma((2,)),
        dma((NZ, 2)), dma((NZ, 2)),
        dma((3,)), dma((3,)),
        dma((4,)),
        dma((2,)), dma((2,)), dma((2,)), dma((2,)),
        dma((3,)), dma((3,)),
        dma((3,)), dma((3,)),
    ]
    return pl.pallas_call(
        kernel,
        out_shape=jax.ShapeDtypeStruct((ROWS, COLS), BF),
        in_specs=[hbm, hbm, hbm, hbm, hbm, hbm],
        out_specs=vmem,
        scratch_shapes=scratch,
        compiler_params=pltpu.CompilerParams(
            collective_id=0, has_side_effects=True, vmem_limit_bytes=53 * 1024 * 1024 + 672 * 1024
        ),
        name="layer",
    )(tokens, query_weight, key_weight, value_weight, out_weight, chosen)


def solution(mesh):
    placed = (P("kv", "tp"), P(None, "tp"), P(None, "tp"), P(None, "tp"), P(None, "tp"), P("kv", None))
    return jax.shard_map(local, mesh=mesh, in_specs=placed, out_specs=P("kv", "tp"), check_vma=False)
```
